512 devices in a mesh: ep: 128 (over z, y, core), tp: 4 (over x).
Axes of the slice: x: 4, y: 8, z: 8, core: 2. Of those that a mesh axis runs over, the one named last changes fastest.
Arguments:
- tokens: bfloat16 [16384, 2048], P('ep'), may hold values from -6 to 6
- norm_gain: float32 [2048], replicated, may hold values from 0.1 to 1.9
- routes: int32 [16384, 2], P('ep'), may hold values from 0 to 127, all different within a row; in each aligned block of 128 rows (0 to 127, 128 to 255, ...) at most 3 rows name the same one
- group_prob: float32 [16384], P('ep'), may hold values from 0.2 to 1
- expert_logits: float32 [16384, 2], P('ep'), may hold values from -6 to 6
- gate_weight: bfloat16 [128, 2048, 384], P('ep', None, 'tp'), may hold values from -0.125 to 0.125
- up_weight: bfloat16 [128, 2048, 384], P('ep', None, 'tp'), may hold values from -0.125 to 0.125
- down_matrix: bfloat16 [128, 384, 2048], P('ep', 'tp'), may hold values from -0.3125 to 0.3125
Outputs:
- combined: bfloat16 [16384, 2048], P('ep', 'tp')
The draws below stay inside these ranges and needn't reach their ends.
Inputs may be any that keep to these rules, and one draw needn't show every extreme that they name: `routes`: each row names 2 different experts. Among the 128 tokens of one index of ep at most 3 rows name one expert, and in every draw some expert is named by exactly 3 of them.
All inputs are finite; a program needn't handle non-finite values.
Results may differ from the reference program's by a relative error of at most 0.013.
Values may be sent and summed in bfloat16 or wider, within the bound.
A program may use at most 64 MiB of HBM per device.

```python
import math
import jax
import jax.numpy as jnp
import numpy as np
from jax import lax

MODEL_DIM = 2048
FF = 384
TOPK = 2
TOK_DEV = 128
EXPERTS = 128
CAP = 3
TOKENS = 16384
N_EP = 128
N_TP = 4


def shard_levels(key, shape, split, least, high):
    level, own = 1.0, jax.random.fold_in(key, 6)
    for axis_at, shards_of in split:
        draws = jnp.exp(jax.random.uniform(jax.random.fold_in(own, axis_at), (shards_of,), jnp.float32, least / len(split), high / len(split)))
        level = level * jnp.repeat(draws, shape[axis_at] // shards_of).reshape([-1 if axis == axis_at else 1 for axis in range(len(shape))])
    return level


def assign_block(stream_key, own, number, rows, number_of, top, limit, lean):
    sequence = jax.random.permutation(stream_key, number_of)
    heavy_load, common = shares(number_of, rows * top, limit, lean, True), shares(number_of, rows * top, limit, lean, False)
    places = jnp.arange(number_of)

    def named(lengths, turn):
        used = int((lengths > 0).sum())
        fixed = max(1, used // 4)
        passed = fixed + (places - fixed + turn * (used - fixed)) % max(1, number_of - fixed)
        return jnp.zeros((number_of,), jnp.int32).at[sequence[jnp.where(places < fixed, places, passed)]].set(jnp.asarray(lengths, jnp.int32))

    lengths = jnp.where(number % 4 == 0, named(heavy_load, number // 4), named(common, number - number // 4 - 1))
    mixed = jax.random.permutation(jax.random.fold_in(own, 3), number_of)
    giver, receiver = mixed[0:number_of // 2 * 2:2], mixed[1:number_of // 2 * 2:2]
    room = jnp.minimum(lengths[giver] - 1, limit - lengths[receiver]) // 2
    room = jnp.where((giver == sequence[0]) | (receiver == sequence[0]) | (lengths[receiver] == 0), 0, jnp.maximum(room, 0))
    passed = jax.random.randint(jax.random.fold_in(own, 4), (number_of // 2,), 0, 1 << 20) % (room + 1)
    lengths = lengths.at[giver].add(-passed).at[receiver].add(passed)
    labels = jnp.searchsorted(jnp.cumsum(lengths), jnp.arange(rows * top), side="right").astype(jnp.int32)
    listing = labels.reshape(top, rows).T
    listing = listing[jax.random.permutation(jax.random.fold_in(own, 1), rows)]
    turn = jax.random.randint(jax.random.fold_in(own, 2), (rows, 1), 0, top)
    return jnp.take_along_axis(listing, (jnp.arange(top)[None, :] + turn) % top, axis=1)


def shares(amount, total, limit, skew, full):
    portions = [(1 << 20) // math.isqrt(standing ** skew) + 1 for standing in range(1, amount + 1)]
    largest = limit if full else min(limit, max(-(-total // amount), total * portions[0] // sum(portions)))
    least = 1 if total - largest >= amount - 1 else 0
    holding, surplus = [largest] + [least] * (amount - 1), total - largest - least * (amount - 1)
    while surplus > 0:
        movable = [i for i in range(1, amount) if holding[i] < largest] or [i for i in range(1, amount) if holding[i] < limit]
        whole, remaining = sum([portions[i] for i in movable]), surplus
        for i in movable:
            extra = min(limit - holding[i], max(1, remaining * portions[i] // whole), surplus)
            holding[i] = holding[i] + extra
            surplus = surplus - extra
    return np.array(holding)


def bell_draw(rng, dims, spread, bound, shards=(), held_as=jnp.bfloat16):
    drawn = spread * jax.random.normal(rng, dims, jnp.float32)
    if shards:
        drawn = drawn * shard_levels(rng, dims, shards, -0.22, 0.18)
    return jnp.clip(drawn, -bound, bound).astype(held_as)


def setup_inputs(seed: int = 0) -> dict:
    key_of = jax.random.split(jax.random.key(seed), 9)
    tokens = bell_draw(key_of[0], (TOKENS, MODEL_DIM), 1.0, 6.0, ((0, 128),))
    norm_gain = jnp.clip(1.0 + 0.18 * jax.random.normal(key_of[1], (MODEL_DIM,), jnp.float32), 0.1, 1.9)
    routes_keys = jax.random.split(jax.random.fold_in(key_of[2], 1), TOKENS // TOK_DEV)
    routes_turns = jax.random.permutation(jax.random.fold_in(key_of[2], 3), TOKENS // TOK_DEV)
    routes = jax.vmap(lambda own, number: assign_block(jax.random.fold_in(key_of[2], 2), own, number, TOK_DEV, EXPERTS, TOPK, CAP, 2))(routes_keys, routes_turns).reshape((TOKENS, TOPK))
    group_prob = jnp.clip(0.2 + 0.8 * jax.random.uniform(key_of[3], (TOKENS,), jnp.float32) ** shard_levels(key_of[3], (TOKENS,), ((0, 128),), -0.2, 0.2), 0.2, 1.0)
    expert_logits = bell_draw(key_of[4], (TOKENS, TOPK), 1.5, 6.0, ((0, 128),), jnp.float32)
    gate_weight = bell_draw(key_of[5], (EXPERTS, MODEL_DIM, FF), MODEL_DIM ** -0.5, 0.125, ((0, 128), (2, 4)))
    up_weight = bell_draw(key_of[6], (EXPERTS, MODEL_DIM, FF), MODEL_DIM ** -0.5, 0.125, ((0, 128), (2, 4)))
    down_matrix = bell_draw(key_of[7], (EXPERTS, FF, MODEL_DIM), FF ** -0.5, 0.3125, ((0, 128), (1, 4)))
    return {"tokens": tokens, "norm_gain": norm_gain, "routes": routes, "group_prob": group_prob, "expert_logits": expert_logits, "gate_weight": gate_weight, "up_weight": up_weight, "down_matrix": down_matrix}


def reference(tokens, norm_gain, routes, group_prob, expert_logits, gate_weight, up_weight, down_matrix):
    values = tokens.astype(jnp.float32)
    normed = (values * lax.rsqrt(lax.optimization_barrier(jnp.mean(values * values, -1, keepdims=True)) + 1e-06) * norm_gain).astype(jnp.bfloat16)
    weights = group_prob[:, None] * jax.nn.softmax(expert_logits.astype(jnp.float32), axis=-1)
    flat_ids = routes.reshape(-1)
    flat_weights = weights.reshape(-1)
    upper_limit = N_EP * CAP
    slice_width = FF // N_TP

    def visit(total, expert_index):
        hits = flat_ids == expert_index
        found = jnp.nonzero(hits, size=upper_limit, fill_value=0)[0].astype(jnp.int32)
        usable = jnp.arange(upper_limit, dtype=jnp.int32) < jnp.sum(hits.astype(jnp.int32))
        owners = (found // TOPK).astype(jnp.int32)
        inputs = normed[owners]
        gate_proj = jnp.dot(inputs, gate_weight[expert_index], preferred_element_type=jnp.float32)
        up_proj = jnp.dot(inputs, up_weight[expert_index], preferred_element_type=jnp.float32)
        hidden_state = (jax.nn.silu(gate_proj) * up_proj).astype(jnp.bfloat16)
        block_list = jnp.einsum('lzn,znx->zlx', hidden_state.reshape(upper_limit, N_TP, slice_width).astype(jnp.float32), down_matrix[expert_index].reshape(N_TP, slice_width, MODEL_DIM).astype(jnp.float32)).astype(jnp.bfloat16)
        expert_out = lax.optimization_barrier(jnp.sum(block_list.astype(jnp.float32), 0)).astype(jnp.bfloat16)
        scale = jnp.where(usable, flat_weights[found], jnp.zeros((), jnp.float32))
        total = total.at[owners].add(expert_out.astype(jnp.float32) * scale[:, None])
        return (total, None)
    total, _ = lax.scan(visit, jnp.zeros((TOKENS, MODEL_DIM), jnp.float32), jnp.arange(EXPERTS, dtype=jnp.int32))
    return total.astype(jnp.bfloat16)
```

```python
import functools

import jax
import jax.numpy as jnp
from jax import lax
from jax.experimental import pallas as pl
from jax.experimental.pallas import tpu as pltpu
from jax.sharding import PartitionSpec as P

MESH = pl.DeviceIdType.MESH
CAP = 3
CORES = 2
F32, BF16 = jnp.float32, jnp.bfloat16


def quotient(values, divisor):
    return lax.shift_right_logical(values * ((65535 + divisor) // divisor), 16)


def far_first(n):
    return sorted(range(1, n), key=lambda d: -min(d, n - d))


def dot(a, b):
    return jnp.dot(a, b, preferred_element_type=F32)


def dot_nt(a, b):
    return lax.dot_general(a, b, (((1,), (1,)), ((), ())), preferred_element_type=F32)


def kernel(
    nz, nyc, ntp,
    tokens, gain, routes, prob, logits, gate, up, down,
    out,
    wg, dn, oa, ob, a1, b1, a1p, b1p, a2, b2, ps, pr, hid, ra, rb, ra1, rb1, ra1p, rb1p, ra2, rb2,
    lsem, wss, wrs, s1s, s1r, s2s, s2r, pss, prs, hss, hrs, s3s, s3r, s4s, s4r, us, ur,
):
    ny = nyc // CORES
    ep, tp = lax.axis_index("ep"), lax.axis_index("tp")
    z, yc = lax.div(ep, nyc), lax.rem(ep, nyc)
    y, core = lax.div(yc, CORES), lax.rem(yc, CORES)
    width = tokens.shape[1]
    share = width // ntp
    half = share // 2
    ff = gate.shape[0]
    experts = nz * nyc
    slots = experts * CAP
    tok = tokens.shape[0]

    z_steps = far_first(nz)
    yc_steps = [(dy, dc) for dy in [*far_first(ny), 0] for dc in range(CORES) if dy or dc]
    x_steps = far_first(ntp)

    def z_to(d):
        return lax.rem(z + d, nz)

    def yc_to(dy, dc):
        return lax.rem(y + dy, ny) * CORES + lax.rem(core + dc, CORES)

    def x_to(d):
        return lax.rem(tp + d, ntp)

    z_peers = [((z_to(d) * nyc + yc, tp), z_to(d), z_to(nz - d), d) for d in z_steps]
    yc_peers = [
        ((z * nyc + yc_to(dy, dc), tp), yc_to(dy, dc), yc_to(ny - dy, dc), dy * CORES + dc)
        for dy, dc in yc_steps
    ]
    x_peers = [((ep, x_to(d)), x_to(d), x_to(ntp - d), d) for d in x_steps]

    barrier = pltpu.get_barrier_semaphore()
    for device, *_ in [*z_peers, *yc_peers, *x_peers]:
        pl.semaphore_signal(barrier, inc=1, device_id=device, device_id_type=MESH)

    pending = []

    def send(src, dst, ssem, rsem, device):
        copy = pltpu.make_async_remote_copy(
            src_ref=src, dst_ref=dst, send_sem=ssem, recv_sem=rsem, device_id=device, device_id_type=MESH
        )
        copy.start()
        pending.append(copy)

    def arrived(dst, ssem, rsem, device):
        pltpu.make_async_remote_copy(
            src_ref=dst, dst_ref=dst, send_sem=ssem, recv_sem=rsem, device_id=device, device_id_type=MESH
        ).wait_recv()

    def exchange(src, dst, peers, mine, ssem, rsem):
        for device, there, _, k in peers:
            send(src.at[there], dst.at[mine], ssem.at[k], rsem.at[k], device)

    def await_all(dst, peers, ssem, rsem):
        for device, _, source, k in peers:
            arrived(dst.at[source], ssem.at[k], rsem.at[k], device)

    def columns(j):
        return pl.ds(pl.multiple_of(j * share, share), share)

    local = [
        pltpu.make_async_copy(gate.at[:, columns(tp)], wg.at[tp, pl.ds(0, ff)], lsem.at[0]),
        pltpu.make_async_copy(up.at[:, columns(tp)], wg.at[tp, pl.ds(ff, ff)], lsem.at[1]),
        pltpu.make_async_copy(down.at[:, columns(tp)], dn.at[tp], lsem.at[2]),
    ]
    for copy in local:
        copy.start()

    r0, r1 = routes[0:1, :], routes[1:2, :]
    ids = lax.broadcasted_iota(jnp.int32, (experts, tok), 0)
    e0, e1 = (ids == r0).astype(F32), (ids == r1).astype(F32)
    before = (
        lax.broadcasted_iota(jnp.int32, (tok, tok), 0) < lax.broadcasted_iota(jnp.int32, (tok, tok), 1)
    ).astype(BF16)
    earlier = dot((e0 + e1).astype(BF16), before)
    c0 = jnp.sum(earlier * e0, 0, keepdims=True).astype(jnp.int32)
    c1 = jnp.sum(earlier * e1, 0, keepdims=True).astype(jnp.int32)

    def by_z(r, c):
        return r * CAP + c

    def by_yc(r, c):
        rz = quotient(r, nyc)
        return ((r - rz * nyc) * nz + rz) * CAP + c

    rows = lax.broadcasted_iota(jnp.int32, (slots, tok), 0)
    at_a0, at_a1 = rows == by_z(r0, c0), rows == by_z(r1, c1)
    at_b0, at_b1 = rows == by_yc(r0, c0), rows == by_yc(r1, c1)

    values = tokens[...].astype(F32)
    scale = lax.rsqrt(jnp.sum(values * values, -1, keepdims=True) * (1.0 / width) + 1e-06)
    normed = (tokens[:, columns(tp)].astype(F32) * scale * gain[:, columns(tp)]).astype(BF16)

    oa[...] = dot((at_a0 | at_a1).astype(BF16), normed[:, :half]).astype(BF16).reshape(oa.shape)
    ob[...] = dot((at_b0 | at_b1).astype(BF16), normed[:, half:]).astype(BF16).reshape(ob.shape)

    pl.semaphore_wait(barrier, len(z_peers) + len(yc_peers) + len(x_peers))

    exchange(oa, a1, z_peers, z, s1s, s1r)
    exchange(ob, b1, yc_peers, yc, s2s, s2r)
    for device, there, _, d in x_peers:
        send(gate.at[:, columns(there)], wg.at[tp, pl.ds(0, ff)], wss.at[0, d], wrs.at[0, d], device)
        send(up.at[:, columns(there)], wg.at[tp, pl.ds(ff, ff)], wss.at[1, d], wrs.at[1, d], device)
    for device, there, _, d in x_peers:
        send(down.at[:, columns(there)], dn.at[tp], wss.at[2, d], wrs.at[2, d], device)
    a1[z] = oa[z]
    b1[yc] = ob[yc]

    top = jnp.maximum(logits[0:1, :], logits[1:2, :])
    x0, x1 = jnp.exp(logits[0:1, :] - top), jnp.exp(logits[1:2, :] - top)
    w0, w1 = prob[...] * (x0 / (x0 + x1)), prob[...] * (x1 / (x0 + x1))
    zero = jnp.zeros((slots, tok), F32)
    wa = (jnp.where(at_a0, w0, zero) + jnp.where(at_a1, w1, zero)).T
    wb = (jnp.where(at_b0, w0, zero) + jnp.where(at_b1, w1, zero)).T
    wa_hi, wb_hi = wa.astype(BF16), wb.astype(BF16)
    wa_lo, wb_lo = (wa - wa_hi.astype(F32)).astype(BF16), (wb - wb_hi.astype(F32)).astype(BF16)

    to = lax.broadcasted_iota(jnp.int32, (slots, slots), 0)
    of = lax.broadcasted_iota(jnp.int32, (slots, slots), 1)

    def reorder(outer, inner):
        i = quotient(to, inner * CAP)
        rest = to - i * (inner * CAP)
        j = quotient(rest, CAP)
        return (of == (j * outer + i) * CAP + (rest - j * CAP)).astype(BF16)

    to_yz, to_zy = reorder(nyc, nz), reorder(nz, nyc)
    same = (of == to).astype(BF16)

    await_all(a1, z_peers, s1s, s1r)
    a1p[...] = dot(to_yz, a1[...].reshape(slots, half)).astype(BF16).reshape(a1p.shape)
    exchange(a1p, a2, yc_peers, yc, s3s.at[0], s3r.at[0])
    a2[yc] = a1p[yc]
    await_all(b1, yc_peers, s2s, s2r)
    b1p[...] = dot(to_zy, b1[...].reshape(slots, half)).astype(BF16).reshape(b1p.shape)
    exchange(b1p, b2, z_peers, z, s4s.at[0], s4r.at[0])
    b2[z] = b1p[z]

    for copy in local:
        copy.wait()
    for device, _, source, d in x_peers:
        arrived(wg.at[source, pl.ds(0, ff)], wss.at[0, d], wrs.at[0, d], device)
        arrived(wg.at[source, pl.ds(ff, ff)], wss.at[1, d], wrs.at[1, d], device)

    await_all(a2, yc_peers, s3s.at[0], s3r.at[0])
    await_all(b2, z_peers, s4s.at[0], s4r.at[0])
    xa = a2[...].reshape(slots, half)
    xb = dot(to_yz, b2[...].reshape(slots, half)).astype(BF16)

    def partial(j):
        return dot_nt(wg[j, :, :half], xa) + dot_nt(wg[j, :, half:], xb)

    for device, there, _, d in x_peers:
        ps[d] = partial(there).astype(BF16)
        send(ps.at[d], pr.at[d], pss.at[d], prs.at[d], device)
    total = partial(tp)
    for device, _, _, d in x_peers:
        arrived(pr.at[d], pss.at[d], prs.at[d], device)
        total = total + pr[d].astype(F32)
    g, u = total[:ff], total[ff:]
    hid[tp] = (g / (1.0 + jnp.exp(-g)) * u).astype(BF16)
    for device, _, _, d in x_peers:
        send(hid.at[tp], hid.at[tp], hss.at[d], hrs.at[d], device)
    for device, _, source, d in x_peers:
        arrived(dn.at[source], wss.at[2, d], wrs.at[2, d], device)
    for device, _, source, d in x_peers:
        arrived(hid.at[source], hss.at[d], hrs.at[d], device)

    hidden = hid[...].reshape(ntp * ff, slots)
    down_all = dn[...].reshape(ntp * ff, share)
    h_yz = dot_nt(same, hidden).astype(BF16)
    ra[...] = dot(h_yz, down_all[:, :half]).astype(BF16).reshape(ra.shape)
    exchange(ra, ra1, yc_peers, yc, s3s.at[1], s3r.at[1])
    ra1[yc] = ra[yc]
    h_zy = dot_nt(to_zy, hidden).astype(BF16)
    rb[...] = dot(h_zy, down_all[:, half:]).astype(BF16).reshape(rb.shape)
    exchange(rb, rb1, z_peers, z, s4s.at[1], s4r.at[1])
    rb1[z] = rb[z]

    await_all(ra1, yc_peers, s3s.at[1], s3r.at[1])
    ra1p[...] = dot(to_zy, ra1[...].reshape(slots, half)).astype(BF16).reshape(ra1p.shape)
    exchange(ra1p, ra2, z_peers, z, us, ur)
    ra2[z] = ra1p[z]
    await_all(rb1, z_peers, s4s.at[1], s4r.at[1])
    rb1p[...] = dot(to_yz, rb1[...].reshape(slots, half)).astype(BF16).reshape(rb1p.shape)
    exchange(rb1p, rb2, yc_peers, yc, s3s.at[2], s3r.at[2])
    rb2[yc] = rb1p[yc]

    await_all(ra2, z_peers, us, ur)
    back = ra2[...].reshape(slots, half)
    out[:, :half] = (dot(wa_hi, back) + dot(wa_lo, back)).astype(BF16)
    await_all(rb2, yc_peers, s3s.at[2], s3r.at[2])
    back = rb2[...].reshape(slots, half)
    out[:, half:] = (dot(wb_hi, back) + dot(wb_lo, back)).astype(BF16)

    for copy in pending:
        copy.wait_send()


def body(nz, tokens, norm_gain, routes, group_prob, expert_logits, gate_weight, up_weight, down_matrix):
    tok, width = tokens.shape
    ntp = lax.axis_size("tp")
    nyc = lax.axis_size("ep") // nz
    share, half = width // ntp, width // ntp // 2
    ff = gate_weight.shape[2]
    slots = nz * nyc * CAP
    by_z = pltpu.VMEM((nz, nyc * CAP, half), BF16)
    by_yc = pltpu.VMEM((nyc, nz * CAP, half), BF16)
    vmem = pl.BlockSpec(memory_space=pltpu.VMEM)
    anywhere = pl.BlockSpec(memory_space=pl.ANY)
    dma = pltpu.SemaphoreType.DMA
    return pl.pallas_call(
        functools.partial(kernel, nz, nyc, ntp),
        out_shape=jax.ShapeDtypeStruct((tok, share), BF16),
        in_specs=[vmem] * 5 + [anywhere] * 3,
        out_specs=vmem,
        scratch_shapes=[
            pltpu.VMEM((ntp, 2 * ff, share), BF16),
            pltpu.VMEM((ntp, ff, share), BF16),
            by_z, by_yc,
            by_z, by_yc,
            by_yc, by_z,
            by_yc, by_z,
            pltpu.VMEM((ntp, 2 * ff, slots), BF16),
            pltpu.VMEM((ntp, 2 * ff, slots), BF16),
            pltpu.VMEM((ntp, ff, slots), BF16),
            by_yc, by_z,
            by_yc, by_z,
            by_z, by_yc,
            by_z, by_yc,
            dma((3,)),
            dma((3, ntp)), dma((3, ntp)),
            dma((nz,)), dma((nz,)),
            dma((nyc,)), dma((nyc,)),
            dma((ntp,)), dma((ntp,)),
            dma((ntp,)), dma((ntp,)),
            dma((3, nyc)), dma((3, nyc)),
            dma((2, nz)), dma((2, nz)),
            dma((nz,)), dma((nz,)),
        ],
        compiler_params=pltpu.CompilerParams(
            collective_id=0, has_side_effects=True, vmem_limit_bytes=40 * 2**20
        ),
    )(
        tokens,
        norm_gain.reshape(1, width),
        routes.T,
        group_prob.reshape(1, tok),
        expert_logits.T,
        jnp.swapaxes(gate_weight, 1, 2)[0],
        jnp.swapaxes(up_weight, 1, 2)[0],
        down_matrix[0],
    )


def solution(mesh, nz=8):
    return jax.shard_map(
        functools.partial(body, nz),
        mesh=mesh,
        in_specs=(
            P("ep", None),
            P(),
            P("ep", None),
            P("ep"),
            P("ep", None),
            P("ep", None, "tp"),
            P("ep", None, "tp"),
            P("ep", "tp", None),
        ),
        out_specs=P("ep", "tp"),
        check_vma=False,
    )
```

```python
import functools

import jax
import jax.numpy as jnp
from jax import lax
from jax.experimental import pallas as pl
from jax.experimental.pallas import tpu as pltpu
from jax.sharding import PartitionSpec as P

MESH = pl.DeviceIdType.MESH
CAP = 3
CORES = 2
F32, BF16 = jnp.float32, jnp.bfloat16
A1, B1, A2, B2, C1, D1, C2, D2, PS, HI, WG = range(0, 11 * CAP, CAP)
DN = WG + 1


def quotient(values, divisor):
    return lax.shift_right_logical(values * ((65535 + divisor) // divisor), 16)


def far_first(n):
    return sorted(range(1, n), key=lambda d: -min(d, n - d))


def dot(a, b):
    return jnp.dot(a, b, preferred_element_type=F32)


def dot_nt(a, b):
    return lax.dot_general(a, b, (((1,), (1,)), ((), ())), preferred_element_type=F32)


def kernel(
    nz, nyc, ntp,
    tokens_hbm, gain_hbm, routes_hbm, prob_hbm, logits_hbm, gate, up, down,
    out,
    tokens, gain, routes, prob, logits,
    wg, dn, oa, ob, a1, b1, a1p, b1p, a2, b2, ps, pr, hid, ra, rb, ra1, rb1, ra1p, rb1p, ra2, rb2,
    lsem, ssem, rsem,
):
    ny = nyc // CORES
    ep, tp = lax.axis_index("ep"), lax.axis_index("tp")
    z, yc = lax.div(ep, nyc), lax.rem(ep, nyc)
    y, core = lax.div(yc, CORES), lax.rem(yc, CORES)
    tok, width = tokens_hbm.shape
    share = width // ntp
    half = share // 2
    ff = gate.shape[0]
    experts = nz * nyc

    z_steps = far_first(nz)
    yc_steps = [(dy, dc) for dy in [*far_first(ny), 0] for dc in range(CORES) if dy or dc]
    x_steps = far_first(ntp)

    def z_to(d):
        return lax.rem(z + d, nz)

    def yc_to(dy, dc):
        return lax.rem(y + dy, ny) * CORES + lax.rem(core + dc, CORES)

    def x_to(d):
        return lax.rem(tp + d, ntp)

    z_peers = [((z_to(d) * nyc + yc, tp), z_to(d), d) for d in z_steps]
    yc_peers = [((z * nyc + yc_to(*d), tp), yc_to(*d), d) for d in yc_steps]
    x_peers = [((ep, x_to(d)), x_to(d), d) for d in x_steps]
    others = pl.ds(1, ntp - 1)

    def columns(j):
        return pl.ds(pl.multiple_of(j * share, share), share)

    inputs = [
        pltpu.make_async_copy(routes_hbm, routes, lsem.at[0]),
        pltpu.make_async_copy(tokens_hbm, tokens, lsem.at[1]),
        pltpu.make_async_copy(gain_hbm.at[:, columns(tp)], gain, lsem.at[2]),
        pltpu.make_async_copy(prob_hbm, prob, lsem.at[3]),
        pltpu.make_async_copy(logits_hbm, logits, lsem.at[4]),
    ]
    for copy in inputs:
        copy.start()

    barrier = pltpu.get_barrier_semaphore()
    for device, *_ in [*z_peers, *yc_peers, *x_peers]:
        pl.semaphore_signal(barrier, inc=1, device_id=device, device_id_type=MESH)

    pending = []

    def remote(src, dst, sems, device):
        return pltpu.make_async_remote_copy(
            src_ref=src, dst_ref=dst, send_sem=sems[0], recv_sem=sems[1], device_id=device, device_id_type=MESH
        )

    def send(src, dst, sems, device):
        remote(src, dst, sems, device).start()

    def pair(number):
        return ssem.at[number], rsem.at[number]

    def exchange(c, src, dst, peers, mine, number):
        sems = pair(number + c)
        for device, there, _ in peers:
            send(src.at[c, there], dst.at[c, mine], sems, device)
        dst[c, mine] = src[c, mine]
        pending.append(remote(src.at[c, pl.ds(0, len(peers))], src.at[c, pl.ds(0, len(peers))], sems, device))

    def await_all(c, dst, peers, number):
        everything = dst.at[c, pl.ds(0, len(peers))]
        remote(everything, everything, pair(number + c), peers[0][0]).wait_recv()

    local = [
        pltpu.make_async_copy(gate.at[:, columns(tp)], wg.at[0, pl.ds(0, ff)], lsem.at[5]),
        pltpu.make_async_copy(up.at[:, columns(tp)], wg.at[0, pl.ds(ff, ff)], lsem.at[6]),
        pltpu.make_async_copy(down.at[:, columns(tp)], dn.at[0], lsem.at[7]),
    ]
    for copy in local:
        copy.start()

    inputs[0].wait()
    r0, r1 = routes[0:1, :], routes[1:2, :]
    ids = lax.broadcasted_iota(jnp.int32, (experts, tok), 0)
    is0, is1 = ids == r0, ids == r1
    e0, e1 = is0.astype(F32), is1.astype(F32)
    before = (
        lax.broadcasted_iota(jnp.int32, (tok, tok), 0) < lax.broadcasted_iota(jnp.int32, (tok, tok), 1)
    ).astype(BF16)
    earlier = dot((e0 + e1).astype(BF16), before)
    c0 = jnp.sum(earlier * e0, 0, keepdims=True)
    c1 = jnp.sum(earlier * e1, 0, keepdims=True)

    def turned(r):
        rz = quotient(r, nyc)
        return (r - rz * nyc) * nz + rz

    is0b, is1b = ids == turned(r0), ids == turned(r1)

    inputs[1].wait()
    inputs[2].wait()
    values = tokens[...].astype(F32)
    scale = lax.rsqrt(jnp.sum(values * values, -1, keepdims=True) * (1.0 / width) + 1e-06)
    normed = (tokens[:, columns(tp)].astype(F32) * scale * gain[...]).astype(BF16)

    for c in range(CAP):
        in0, in1 = c0 == c, c1 == c
        pick = ((is0 & in0) | (is1 & in1)).astype(BF16)
        oa[c] = dot(pick, normed[:, :half]).astype(BF16).reshape(oa.shape[1:])
        pick = ((is0b & in0) | (is1b & in1)).astype(BF16)
        ob[c] = dot(pick, normed[:, half:]).astype(BF16).reshape(ob.shape[1:])

    pl.semaphore_wait(barrier, len(z_peers) + len(yc_peers) + len(x_peers))

    for c in range(CAP):
        exchange(c, oa, a1, z_peers, z, A1)
        exchange(c, ob, b1, yc_peers, yc, B1)
        if c == 0:
            for device, there, d in x_peers:
                send(gate.at[:, columns(there)], wg.at[d, pl.ds(0, ff)], pair(WG), device)
                send(up.at[:, columns(there)], wg.at[d, pl.ds(ff, ff)], pair(WG), device)
            gates_and_ups = remote(wg.at[others], wg.at[others], pair(WG), device)
    for device, there, d in x_peers:
        send(down.at[:, columns(there)], dn.at[d], pair(DN), device)
    downs = remote(dn.at[others], dn.at[others], pair(DN), device)
    pending += [gates_and_ups, downs]

    to = lax.broadcasted_iota(jnp.int32, (experts, experts), 0)
    of = lax.broadcasted_iota(jnp.int32, (experts, experts), 1)

    def reorder(outer, inner):
        i = quotient(to, inner)
        return (of == (to - i * inner) * outer + i).astype(BF16)

    to_yz, to_zy = reorder(nyc, nz), reorder(nz, nyc)
    same = (of == to).astype(BF16)

    def reordered(c, matrix, src, dst):
        dst[c] = dot(matrix, src[c].reshape(experts, half)).astype(BF16).reshape(dst.shape[1:])

    for c in range(CAP):
        await_all(c, a1, z_peers, A1)
        reordered(c, to_yz, a1, a1p)
        exchange(c, a1p, a2, yc_peers, yc, A2)
        await_all(c, b1, yc_peers, B1)
        reordered(c, to_zy, b1, b1p)
        exchange(c, b1p, b2, z_peers, z, B2)

    inputs[3].wait()
    inputs[4].wait()
    top = jnp.maximum(logits[0:1, :], logits[1:2, :])
    x0, x1 = jnp.exp(logits[0:1, :] - top), jnp.exp(logits[1:2, :] - top)
    w0, w1 = prob[...] * (x0 / (x0 + x1)), prob[...] * (x1 / (x0 + x1))
    zero = jnp.zeros((experts, tok), F32)

    def split(at0, at1):
        whole = (jnp.where(at0, w0, zero) + jnp.where(at1, w1, zero)).T
        high = whole.astype(BF16)
        return high, (whole - high.astype(F32)).astype(BF16)

    mix_a = [split(is0 & (c0 == c), is1 & (c1 == c)) for c in range(CAP)]
    mix_b = [split(is0b & (c0 == c), is1b & (c1 == c)) for c in range(CAP)]

    for copy in local:
        copy.wait()
    gates_and_ups.wait_recv()

    own = []
    for c in range(CAP):
        await_all(c, a2, yc_peers, A2)
        await_all(c, b2, z_peers, B2)
        xa = a2[c].reshape(experts, half)
        xb = dot(to_yz, b2[c].reshape(experts, half)).astype(BF16)

        def partial(d):
            return dot_nt(wg[d, :, :half], xa) + dot_nt(wg[d, :, half:], xb)

        for device, _, d in x_peers:
            ps[c, d] = partial(ntp - d).astype(BF16)
            send(ps.at[c, d], pr.at[c, d], pair(PS + c), device)
        pending.append(remote(ps.at[c, others], pr.at[c, others], pair(PS + c), device))
        own.append((partial(0), pending[-1]))

    blocks = []
    for c in range(CAP):
        total, parts = own[c]
        parts.wait_recv()
        for d in range(1, ntp):
            total = total + pr[c, d].astype(F32)
        g, u = total[:ff], total[ff:]
        hid[c, 0] = (g / (1.0 + jnp.exp(-g)) * u).astype(BF16)
        for device, _, d in x_peers:
            send(hid.at[c, 0], hid.at[c, d], pair(HI + c), device)
        blocks.append(remote(hid.at[c, others], hid.at[c, others], pair(HI + c), device))
    pending += blocks

    downs.wait_recv()
    down_all = dn[...].reshape(ntp * ff, share)

    for c in range(CAP):
        blocks[c].wait_recv()
        hidden = hid[c].reshape(ntp * ff, experts)
        h_yz = dot_nt(same, hidden).astype(BF16)
        ra[c] = dot(h_yz, down_all[:, :half]).astype(BF16).reshape(ra.shape[1:])
        exchange(c, ra, ra1, yc_peers, yc, C1)
        h_zy = dot_nt(to_zy, hidden).astype(BF16)
        rb[c] = dot(h_zy, down_all[:, half:]).astype(BF16).reshape(rb.shape[1:])
        exchange(c, rb, rb1, z_peers, z, D1)

    for c in range(CAP):
        await_all(c, ra1, yc_peers, C1)
        reordered(c, to_zy, ra1, ra1p)
        exchange(c, ra1p, ra2, z_peers, z, C2)
        await_all(c, rb1, z_peers, D1)
        reordered(c, to_yz, rb1, rb1p)
        exchange(c, rb1p, rb2, yc_peers, yc, D2)

    sum_a, sum_b = 0.0, 0.0
    for c in range(CAP):
        await_all(c, ra2, z_peers, C2)
        back = ra2[c].reshape(experts, half)
        sum_a = sum_a + (dot(mix_a[c][0], back) + dot(mix_a[c][1], back))
        await_all(c, rb2, yc_peers, D2)
        back = rb2[c].reshape(experts, half)
        sum_b = sum_b + (dot(mix_b[c][0], back) + dot(mix_b[c][1], back))
    out[:, :half] = sum_a.astype(BF16)
    out[:, half:] = sum_b.astype(BF16)

    for copy in pending:
        copy.wait_send()


def body(nz, tokens, norm_gain, routes, group_prob, expert_logits, gate_weight, up_weight, down_matrix):
    tok, width = tokens.shape
    ntp = lax.axis_size("tp")
    nyc = lax.axis_size("ep") // nz
    share, half = width // ntp, width // ntp // 2
    ff = gate_weight.shape[2]
    experts = nz * nyc
    by_z = pltpu.VMEM((CAP, nz, nyc, half), BF16)
    by_yc = pltpu.VMEM((CAP, nyc, nz, half), BF16)
    dma = pltpu.SemaphoreType.DMA
    return pl.pallas_call(
        functools.partial(kernel, nz, nyc, ntp),
        out_shape=jax.ShapeDtypeStruct((tok, share), BF16),
        in_specs=[pl.BlockSpec(memory_space=pltpu.HBM)] * 8,
        out_specs=pl.BlockSpec(memory_space=pltpu.VMEM),
        scratch_shapes=[
            pltpu.VMEM((tok, width), BF16),
            pltpu.VMEM((1, share), F32),
            pltpu.VMEM((2, tok), jnp.int32),
            pltpu.VMEM((1, tok), F32),
            pltpu.VMEM((2, tok), F32),
            pltpu.VMEM((ntp, 2 * ff, share), BF16),
            pltpu.VMEM((ntp, ff, share), BF16),
            by_z, by_yc,
            by_z, by_yc,
            by_yc, by_z,
            by_yc, by_z,
            pltpu.VMEM((CAP, ntp, 2 * ff, experts), BF16),
            pltpu.VMEM((CAP, ntp, 2 * ff, experts), BF16),
            pltpu.VMEM((CAP, ntp, ff, experts), BF16),
            by_yc, by_z,
            by_yc, by_z,
            by_z, by_yc,
            by_z, by_yc,
            dma((8,)),
            dma((DN + 1,)), dma((DN + 1,)),
        ],
        compiler_params=pltpu.CompilerParams(
            collective_id=0, has_side_effects=True, vmem_limit_bytes=67043328
        ),
    )(
        tokens,
        norm_gain.reshape(1, width),
        routes.T,
        group_prob.reshape(1, tok),
        expert_logits.T,
        jnp.swapaxes(gate_weight, 1, 2)[0],
        jnp.swapaxes(up_weight, 1, 2)[0],
        down_matrix[0],
    )


def solution(mesh, nz=8):
    return jax.shard_map(
        functools.partial(body, nz),
        mesh=mesh,
        in_specs=(
            P("ep", None),
            P(),
            P("ep", None),
            P("ep"),
            P("ep", None),
            P("ep", None, "tp"),
            P("ep", None, "tp"),
            P("ep", "tp", None),
        ),
        out_specs=P("ep", "tp"),
        check_vma=False,
    )
```

```python
import functools

import jax
import jax.numpy as jnp
from jax import lax
from jax.experimental import pallas as pl
from jax.experimental.pallas import tpu as pltpu
from jax.sharding import PartitionSpec as P

MESH = pl.DeviceIdType.MESH
CAP = 3
CORES = 2
F32, BF16 = jnp.float32, jnp.bfloat16
A1, B1, A2, B2, C1, D1, C2, D2, PS, HI, WG = range(0, 11 * CAP, CAP)
DN = WG + 1
CHUNKS = ((0, 0), (0, 1)), ((1, 0), (2, 0)), ((1, 1), (2, 1))


def quotient(values, divisor):
    return lax.shift_right_logical(values * ((65535 + divisor) // divisor), 16)


def far_first(n):
    return sorted(range(1, n), key=lambda d: -min(d, n - d))


def dot(a, b):
    return jnp.dot(a, b, preferred_element_type=F32)


def dot_nt(a, b):
    return lax.dot_general(a, b, (((1,), (1,)), ((), ())), preferred_element_type=F32)


def kernel(
    nz, nyc, ntp,
    tokens_hbm, gain_hbm, routes_hbm, prob_hbm, logits_hbm, gate, up, down,
    out,
    tokens, gain, routes, prob, logits,
    wg, dn, oa, ob, a1, b1, a1p, b1p, a2, b2, ps, pr, hid, ra, rb, ra1, rb1, ra1p, rb1p, ra2, rb2,
    lsem, ssem, rsem,
):
    ny = nyc // CORES
    ep, tp = lax.axis_index("ep"), lax.axis_index("tp")
    z, yc = lax.div(ep, nyc), lax.rem(ep, nyc)
    y, core = lax.div(yc, CORES), lax.rem(yc, CORES)
    tok, width = tokens_hbm.shape
    share = width // ntp
    half = share // 2
    ff = gate.shape[0]
    experts = nz * nyc
    side, rows = nz // 2, experts // 2

    z_steps = far_first(nz)
    yc_steps = [(dy, dc) for dy in [*far_first(ny), 0] for dc in range(CORES) if dy or dc]
    x_steps = far_first(ntp)

    def z_to(d):
        return lax.rem(z + d, nz)

    def yc_to(dy, dc):
        return lax.rem(y + dy, ny) * CORES + lax.rem(core + dc, CORES)

    def x_to(d):
        return lax.rem(tp + d, ntp)

    z_peers = [((z_to(d) * nyc + yc, tp), z_to(d), d) for d in z_steps]
    yc_peers = [((z * nyc + yc_to(*d), tp), yc_to(*d), d) for d in yc_steps]
    x_peers = [((ep, x_to(d)), x_to(d), d) for d in x_steps]
    others = pl.ds(1, ntp - 1)

    def columns(j):
        return pl.ds(pl.multiple_of(j * share, share), share)

    inputs = [
        pltpu.make_async_copy(routes_hbm, routes, lsem.at[0]),
        pltpu.make_async_copy(tokens_hbm, tokens, lsem.at[1]),
        pltpu.make_async_copy(gain_hbm.at[:, columns(tp)], gain, lsem.at[2]),
        pltpu.make_async_copy(prob_hbm, prob, lsem.at[3]),
        pltpu.make_async_copy(logits_hbm, logits, lsem.at[4]),
    ]
    for copy in inputs:
        copy.start()

    barrier = pltpu.get_barrier_semaphore()
    for device, *_ in [*z_peers, *yc_peers, *x_peers]:
        pl.semaphore_signal(barrier, inc=1, device_id=device, device_id_type=MESH)

    pending = []

    def remote(src, dst, sems, device):
        return pltpu.make_async_remote_copy(
            src_ref=src, dst_ref=dst, send_sem=sems[0], recv_sem=sems[1], device_id=device, device_id_type=MESH
        )

    def send(src, dst, sems, device):
        remote(src, dst, sems, device).start()

    def pair(number):
        return ssem.at[number], rsem.at[number]

    def exchange(c, src, dst, peers, mine, number):
        sems = pair(number + c)
        for device, there, _ in peers:
            send(src.at[c, there], dst.at[c, mine], sems, device)
        dst[c, mine] = src[c, mine]
        pending.append(remote(src.at[c, pl.ds(0, len(peers))], src.at[c, pl.ds(0, len(peers))], sems, device))

    def await_all(c, dst, peers, number):
        everything = dst.at[c, pl.ds(0, len(peers))]
        remote(everything, everything, pair(number + c), peers[0][0]).wait_recv()

    local = [
        pltpu.make_async_copy(gate.at[:, columns(tp)], wg.at[0, pl.ds(0, ff)], lsem.at[5]),
        pltpu.make_async_copy(up.at[:, columns(tp)], wg.at[0, pl.ds(ff, ff)], lsem.at[6]),
        pltpu.make_async_copy(down.at[:, columns(tp)], dn.at[0], lsem.at[7]),
    ]
    for copy in local:
        copy.start()

    inputs[0].wait()
    r0, r1 = routes[0:1, :], routes[1:2, :]
    ids = lax.broadcasted_iota(jnp.int32, (experts, tok), 0)
    is0, is1 = ids == r0, ids == r1
    e0, e1 = is0.astype(F32), is1.astype(F32)
    before = (
        lax.broadcasted_iota(jnp.int32, (tok, tok), 0) < lax.broadcasted_iota(jnp.int32, (tok, tok), 1)
    ).astype(BF16)
    earlier = dot((e0 + e1).astype(BF16), before)
    c0 = jnp.sum(earlier * e0, 0, keepdims=True)
    c1 = jnp.sum(earlier * e1, 0, keepdims=True)

    def turned(r):
        rz = quotient(r, nyc)
        return (r - rz * nyc) * nz + rz

    is0b, is1b = ids == turned(r0), ids == turned(r1)

    inputs[1].wait()
    inputs[2].wait()
    values = tokens[...].astype(F32)
    scale = lax.rsqrt(jnp.sum(values * values, -1, keepdims=True) * (1.0 / width) + 1e-06)
    normed = (tokens[:, columns(tp)].astype(F32) * scale * gain[...]).astype(BF16)

    for c in range(CAP):
        in0, in1 = c0 == c, c1 == c
        pick = ((is0 & in0) | (is1 & in1)).astype(BF16)
        oa[c] = dot(pick, normed[:, :half]).astype(BF16).reshape(oa.shape[1:])
        pick = ((is0b & in0) | (is1b & in1)).astype(BF16)
        ob[c] = dot(pick, normed[:, half:]).astype(BF16).reshape(ob.shape[1:])

    pl.semaphore_wait(barrier, len(z_peers) + len(yc_peers) + len(x_peers))

    for c in range(CAP):
        exchange(c, oa, a1, z_peers, z, A1)
        exchange(c, ob, b1, yc_peers, yc, B1)
        if c == 0:
            for device, there, d in x_peers:
                send(gate.at[:, columns(there)], wg.at[d, pl.ds(0, ff)], pair(WG), device)
                send(up.at[:, columns(there)], wg.at[d, pl.ds(ff, ff)], pair(WG), device)
            gates_and_ups = remote(wg.at[others], wg.at[others], pair(WG), device)
    for device, there, d in x_peers:
        send(down.at[:, columns(there)], dn.at[d], pair(DN), device)
    downs = remote(dn.at[others], dn.at[others], pair(DN), device)
    pending += [gates_and_ups, downs]

    to = lax.broadcasted_iota(jnp.int32, (experts, experts), 0)
    of = lax.broadcasted_iota(jnp.int32, (experts, experts), 1)

    def reorder(outer, inner):
        i = quotient(to, inner)
        return (of == (to - i * inner) * outer + i).astype(BF16)

    to_yz, to_zy = reorder(nyc, nz), reorder(nz, nyc)
    same = (of == to).astype(BF16)

    def reordered(c, matrix, src, dst):
        dst[c] = dot(matrix, src[c].reshape(experts, half)).astype(BF16).reshape(dst.shape[1:])

    for c in range(CAP):
        await_all(c, a1, z_peers, A1)
        reordered(c, to_yz, a1, a1p)
        exchange(c, a1p, a2, yc_peers, yc, A2)
        await_all(c, b1, yc_peers, B1)
        reordered(c, to_zy, b1, b1p)
        exchange(c, b1p, b2, z_peers, z, B2)

    inputs[3].wait()
    inputs[4].wait()
    top = jnp.maximum(logits[0:1, :], logits[1:2, :])
    x0, x1 = jnp.exp(logits[0:1, :] - top), jnp.exp(logits[1:2, :] - top)
    w0, w1 = prob[...] * (x0 / (x0 + x1)), prob[...] * (x1 / (x0 + x1))
    zero = jnp.zeros((experts, tok), F32)

    def split(at0, at1):
        whole = (jnp.where(at0, w0, zero) + jnp.where(at1, w1, zero)).T
        high = whole.astype(BF16)
        return high, (whole - high.astype(F32)).astype(BF16)

    mix_a = [split(is0 & (c0 == c), is1 & (c1 == c)) for c in range(CAP)]
    mix_b = [split(is0b & (c0 == c), is1b & (c1 == c)) for c in range(CAP)]

    for copy in local:
        copy.wait()
    gates_and_ups.wait_recv()

    own, here = [], set()
    for k, blocks in enumerate(CHUNKS):
        for c in sorted({c for c, _ in blocks} - here):
            await_all(c, a2, yc_peers, A2)
            await_all(c, b2, z_peers, B2)
            here.add(c)
        xa = [
            dot(to_zy[h * rows : (h + 1) * rows], a2[c].reshape(experts, half)).astype(BF16) for c, h in blocks
        ]
        xb = [b2[c, pl.ds(h * side, side)].reshape(rows, half) for c, h in blocks]
        xa, xb = jnp.concatenate(xa, 0), jnp.concatenate(xb, 0)

        def partial(d):
            return dot_nt(wg[d, :, :half], xa) + dot_nt(wg[d, :, half:], xb)

        for device, _, d in x_peers:
            ps[k, d] = partial(ntp - d).astype(BF16)
            send(ps.at[k, d], pr.at[k, d], pair(PS + k), device)
        pending.append(remote(ps.at[k, others], pr.at[k, others], pair(PS + k), device))
        own.append((partial(0), pending[-1]))

    gathered = []
    for k in range(CAP):
        total, parts = own[k]
        parts.wait_recv()
        for d in range(1, ntp):
            total = total + pr[k, d].astype(F32)
        g, u = total[:ff], total[ff:]
        hid[k, 0] = (g / (1.0 + jnp.exp(-g)) * u).astype(BF16)
        for device, _, d in x_peers:
            send(hid.at[k, 0], hid.at[k, d], pair(HI + k), device)
        gathered.append(remote(hid.at[k, others], hid.at[k, others], pair(HI + k), device))
    pending += gathered

    def to_halves(k, src, dst, number):
        for b, (c, h) in enumerate(CHUNKS[k]):
            for j in range(side):
                there = h * side + j

                @pl.when(z != there)
                def _(b=b, c=c, j=j, there=there):
                    send(src.at[k, b * side + j], dst.at[c, z], pair(number + c), (there * nyc + yc, tp))

                @pl.when(z == there)
                def _(b=b, c=c, j=j, there=there):
                    dst[c, there] = src[k, b * side + j]

    downs.wait_recv()
    down_all = dn[...].reshape(ntp * ff, share)

    for k in range(CAP):
        gathered[k].wait_recv()
        hidden = hid[k].reshape(ntp * ff, experts)
        h_yz = dot_nt(to_yz, hidden).astype(BF16)
        ra[k] = dot(h_yz, down_all[:, :half]).astype(BF16).reshape(ra.shape[1:])
        exchange(k, ra, ra1, yc_peers, yc, C1)
        h_zy = dot_nt(same, hidden).astype(BF16)
        rb[k] = dot(h_zy, down_all[:, half:]).astype(BF16).reshape(rb.shape[1:])
        to_halves(k, rb, rb1, D1)

    def forward_a(k):
        await_all(k, ra1, yc_peers, C1)
        reordered(k, to_zy, ra1, ra1p)
        to_halves(k, ra1p, ra2, C2)

    def forward_b(*slots):
        for c in slots:
            await_all(c, rb1, z_peers, D1)
            reordered(c, to_yz, rb1, rb1p)
            for device, there, _ in yc_peers:
                send(rb1p.at[c, there], rb2.at[c, yc], pair(D2 + c), device)
            rb2[c, yc] = rb1p[c, yc]

    def in_half(h):
        return lax.div(z, side) == h

    for k, blocks in enumerate(CHUNKS):
        forward_a(k)
        for h in range(2):
            slots = [c for c, of_half in blocks if of_half == h]
            if slots:
                pl.when(in_half(h))(functools.partial(forward_b, *slots))
    for c in range(CAP):
        for src, peers, number in ((rb, z_peers, D1), (ra1p, z_peers, C2), (rb1p, yc_peers, D2)):
            everything = src.at[c, pl.ds(0, len(peers))]
            pending.append(remote(everything, everything, pair(number + c), peers[0][0]))

    sum_a, sum_b = 0.0, 0.0
    for c in range(CAP):
        await_all(c, ra2, z_peers, C2)
        back = ra2[c].reshape(experts, half)
        sum_a = sum_a + (dot(mix_a[c][0], back) + dot(mix_a[c][1], back))
        await_all(c, rb2, yc_peers, D2)
        back = rb2[c].reshape(experts, half)
        sum_b = sum_b + (dot(mix_b[c][0], back) + dot(mix_b[c][1], back))
    out[:, :half] = sum_a.astype(BF16)
    out[:, half:] = sum_b.astype(BF16)

    for copy in pending:
        copy.wait_send()


def body(nz, tokens, norm_gain, routes, group_prob, expert_logits, gate_weight, up_weight, down_matrix):
    tok, width = tokens.shape
    ntp = lax.axis_size("tp")
    nyc = lax.axis_size("ep") // nz
    share, half = width // ntp, width // ntp // 2
    ff = gate_weight.shape[2]
    experts = nz * nyc
    by_z = pltpu.VMEM((CAP, nz, nyc, half), BF16)
    by_yc = pltpu.VMEM((CAP, nyc, nz, half), BF16)
    dma = pltpu.SemaphoreType.DMA
    return pl.pallas_call(
        functools.partial(kernel, nz, nyc, ntp),
        out_shape=jax.ShapeDtypeStruct((tok, share), BF16),
        in_specs=[pl.BlockSpec(memory_space=pltpu.HBM)] * 8,
        out_specs=pl.BlockSpec(memory_space=pltpu.VMEM),
        scratch_shapes=[
            pltpu.VMEM((tok, width), BF16),
            pltpu.VMEM((1, share), F32),
            pltpu.VMEM((2, tok), jnp.int32),
            pltpu.VMEM((1, tok), F32),
            pltpu.VMEM((2, tok), F32),
            pltpu.VMEM((ntp, 2 * ff, share), BF16),
            pltpu.VMEM((ntp, ff, share), BF16),
            by_z, by_yc,
            by_z, by_yc,
            by_yc, by_z,
            by_yc, by_z,
            pltpu.VMEM((CAP, ntp, 2 * ff, experts), BF16),
            pltpu.VMEM((CAP, ntp, 2 * ff, experts), BF16),
            pltpu.VMEM((CAP, ntp, ff, experts), BF16),
            by_yc, by_z,
            by_yc, by_z,
            by_z, by_yc,
            by_z, by_yc,
            dma((8,)),
            dma((DN + 1,)), dma((DN + 1,)),
        ],
        compiler_params=pltpu.CompilerParams(
            collective_id=0, has_side_effects=True, vmem_limit_bytes=40 * 2**20
        ),
    )(
        pltpu.with_memory_space_constraint(tokens, pltpu.HBM),
        pltpu.with_memory_space_constraint(norm_gain.reshape(1, width), pltpu.HBM),
        pltpu.with_memory_space_constraint(routes.T, pltpu.HBM),
        pltpu.with_memory_space_constraint(group_prob.reshape(1, tok), pltpu.HBM),
        pltpu.with_memory_space_constraint(expert_logits.T, pltpu.HBM),
        pltpu.with_memory_space_constraint(jnp.swapaxes(gate_weight, 1, 2)[0], pltpu.HBM),
        pltpu.with_memory_space_constraint(jnp.swapaxes(up_weight, 1, 2)[0], pltpu.HBM),
        pltpu.with_memory_space_constraint(down_matrix[0], pltpu.HBM),
    )


def solution(mesh, nz=8):
    return jax.shard_map(
        functools.partial(body, nz),
        mesh=mesh,
        in_specs=(
            P("ep", None),
            P(),
            P("ep", None),
            P("ep"),
            P("ep", None),
            P("ep", None, "tp"),
            P("ep", None, "tp"),
            P("ep", "tp", None),
        ),
        out_specs=P("ep", "tp"),
        check_vma=False,
    )
```

```python
import functools

import jax
import jax.numpy as jnp
from jax import lax
from jax.experimental import pallas as pl
from jax.experimental.pallas import tpu as pltpu
from jax.sharding import PartitionSpec as P

MESH = pl.DeviceIdType.MESH
CAP = 3
CORES = 2
F32, BF16 = jnp.float32, jnp.bfloat16
A1, B1, A2, B2, RE = range(0, 5 * CAP, CAP)
CHUNKS = ((0, 0), (0, 1)), ((1, 0), (2, 0)), ((1, 1),), ((2, 1),)
NK = len(CHUNKS)
ORDER = [
    ("start", 0),
    ("start", 1),
    ("start", 2),
    ("finish", 0),
    ("finish", 1),
    ("start", 3),
    ("finish", 2),
    ("down", 0),
    ("down", 1),
    ("finish", 3),
    ("down", 2),
    ("down", 3),
]
PS, HI, WG = range(5 * CAP, 5 * CAP + 3 * NK, NK)
DN = WG + 1


def quotient(values, divisor):
    return lax.shift_right_logical(values * ((65535 + divisor) // divisor), 16)


def far_first(n):
    return sorted(range(1, n), key=lambda d: -min(d, n - d))


def dot(a, b):
    return jnp.dot(a, b, preferred_element_type=F32)


def dot_nt(a, b):
    return lax.dot_general(a, b, (((1,), (1,)), ((), ())), preferred_element_type=F32)


def kernel(
    nz, nyc, ntp,
    tokens_hbm, gain_hbm, routes_hbm, prob_hbm, logits_hbm, gate, up, down,
    out,
    tokens, gain, routes, prob, logits,
    wg, dn, oa, ob, a1, b1, a1p, b1p, a2, b2, ps, pr, hid, leaving, back,
    lsem, ssem, rsem,
):
    ny = nyc // CORES
    ep, tp = lax.axis_index("ep"), lax.axis_index("tp")
    z, yc = lax.div(ep, nyc), lax.rem(ep, nyc)
    y, core = lax.div(yc, CORES), lax.rem(yc, CORES)
    tok, width = tokens_hbm.shape
    share = width // ntp
    half = share // 2
    ff = gate.shape[0]
    experts = nz * nyc
    side, rows = nz // 2, experts // 2

    z_steps = far_first(nz)
    yc_steps = [(dy, dc) for dy in [*far_first(ny), 0] for dc in range(CORES) if dy or dc]
    x_steps = far_first(ntp)

    def z_to(d):
        return lax.rem(z + d, nz)

    def yc_to(dy, dc):
        return lax.rem(y + dy, ny) * CORES + lax.rem(core + dc, CORES)

    def x_to(d):
        return lax.rem(tp + d, ntp)

    z_peers = [((z_to(d) * nyc + yc, tp), z_to(d), d) for d in z_steps]
    yc_peers = [((z * nyc + yc_to(*d), tp), yc_to(*d), d) for d in yc_steps]
    x_peers = [((ep, x_to(d)), x_to(d), d) for d in x_steps]
    others = pl.ds(1, ntp - 1)

    def columns(j):
        return pl.ds(pl.multiple_of(j * share, share), share)

    inputs = [
        pltpu.make_async_copy(routes_hbm, routes, lsem.at[0]),
        pltpu.make_async_copy(tokens_hbm, tokens, lsem.at[1]),
        pltpu.make_async_copy(gain_hbm.at[:, columns(tp)], gain, lsem.at[2]),
        pltpu.make_async_copy(prob_hbm, prob, lsem.at[3]),
        pltpu.make_async_copy(logits_hbm, logits, lsem.at[4]),
    ]
    for copy in inputs:
        copy.start()

    barrier = pltpu.get_barrier_semaphore()
    for device, *_ in [*z_peers, *yc_peers, *x_peers]:
        pl.semaphore_signal(barrier, inc=1, device_id=device, device_id_type=MESH)

    pending = []

    def remote(src, dst, sems, device):
        return pltpu.make_async_remote_copy(
            src_ref=src, dst_ref=dst, send_sem=sems[0], recv_sem=sems[1], device_id=device, device_id_type=MESH
        )

    def send(src, dst, sems, device):
        remote(src, dst, sems, device).start()

    def pair(number):
        return ssem.at[number], rsem.at[number]

    def exchange(c, src, dst, peers, mine, number):
        sems = pair(number + c)
        for device, there, _ in peers:
            send(src.at[c, there], dst.at[c, mine], sems, device)
        dst[c, mine] = src[c, mine]
        pending.append(remote(src.at[c, pl.ds(0, len(peers))], src.at[c, pl.ds(0, len(peers))], sems, device))

    def await_all(c, dst, peers, number):
        everything = dst.at[c, pl.ds(0, len(peers))]
        remote(everything, everything, pair(number + c), peers[0][0]).wait_recv()

    local = [
        pltpu.make_async_copy(gate.at[:, columns(tp)], wg.at[0, pl.ds(0, ff)], lsem.at[5]),
        pltpu.make_async_copy(up.at[:, columns(tp)], wg.at[0, pl.ds(ff, ff)], lsem.at[6]),
        pltpu.make_async_copy(down.at[:, columns(tp)], dn.at[0], lsem.at[7]),
    ]
    for copy in local:
        copy.start()

    inputs[0].wait()
    r0, r1 = routes[0:1, :], routes[1:2, :]
    ids = lax.broadcasted_iota(jnp.int32, (experts, tok), 0)
    is0, is1 = ids == r0, ids == r1
    e0, e1 = is0.astype(F32), is1.astype(F32)
    before = (
        lax.broadcasted_iota(jnp.int32, (tok, tok), 0) < lax.broadcasted_iota(jnp.int32, (tok, tok), 1)
    ).astype(BF16)
    earlier = dot((e0 + e1).astype(BF16), before)
    c0 = jnp.sum(earlier * e0, 0, keepdims=True)
    c1 = jnp.sum(earlier * e1, 0, keepdims=True)

    def turned(r):
        rz = quotient(r, nyc)
        return (r - rz * nyc) * nz + rz

    is0b, is1b = ids == turned(r0), ids == turned(r1)

    inputs[1].wait()
    inputs[2].wait()
    values = tokens[...].astype(F32)
    scale = lax.rsqrt(jnp.sum(values * values, -1, keepdims=True) * (1.0 / width) + 1e-06)
    normed = (tokens[:, columns(tp)].astype(F32) * scale * gain[...]).astype(BF16)

    for c in range(CAP):
        in0, in1 = c0 == c, c1 == c
        pick = ((is0 & in0) | (is1 & in1)).astype(BF16)
        oa[c] = dot(pick, normed[:, :half]).astype(BF16).reshape(oa.shape[1:])
        pick = ((is0b & in0) | (is1b & in1)).astype(BF16)
        ob[c] = dot(pick, normed[:, half:]).astype(BF16).reshape(ob.shape[1:])

    pl.semaphore_wait(barrier, len(z_peers) + len(yc_peers) + len(x_peers))

    for c in range(CAP):
        exchange(c, oa, a1, z_peers, z, A1)
        exchange(c, ob, b1, yc_peers, yc, B1)
        if c == 0:
            for device, there, d in x_peers:
                send(gate.at[:, columns(there)], wg.at[d, pl.ds(0, ff)], pair(WG), device)
                send(up.at[:, columns(there)], wg.at[d, pl.ds(ff, ff)], pair(WG), device)
            gates_and_ups = remote(wg.at[others], wg.at[others], pair(WG), device)
    for device, there, d in x_peers:
        send(down.at[:, columns(there)], dn.at[d], pair(DN), device)
    downs = remote(dn.at[others], dn.at[others], pair(DN), device)
    pending += [gates_and_ups, downs]

    to = lax.broadcasted_iota(jnp.int32, (experts, experts), 0)
    of = lax.broadcasted_iota(jnp.int32, (experts, experts), 1)

    def reorder(outer, inner):
        i = quotient(to, inner)
        return (of == (to - i * inner) * outer + i).astype(BF16)

    to_yz, to_zy = reorder(nyc, nz), reorder(nz, nyc)
    same = (of == to).astype(BF16)

    def reordered(c, matrix, src, dst):
        dst[c] = dot(matrix, src[c].reshape(experts, half)).astype(BF16).reshape(dst.shape[1:])

    for c in range(CAP):
        await_all(c, a1, z_peers, A1)
        reordered(c, to_yz, a1, a1p)
        exchange(c, a1p, a2, yc_peers, yc, A2)
        await_all(c, b1, yc_peers, B1)
        reordered(c, to_zy, b1, b1p)
        exchange(c, b1p, b2, z_peers, z, B2)

    inputs[3].wait()
    inputs[4].wait()
    top = jnp.maximum(logits[0:1, :], logits[1:2, :])
    x0, x1 = jnp.exp(logits[0:1, :] - top), jnp.exp(logits[1:2, :] - top)
    w0, w1 = prob[...] * (x0 / (x0 + x1)), prob[...] * (x1 / (x0 + x1))
    zero = jnp.zeros((experts, tok), F32)

    def split(at0, at1):
        whole = (jnp.where(at0, w0, zero) + jnp.where(at1, w1, zero)).T
        high = whole.astype(BF16)
        return high, (whole - high.astype(F32)).astype(BF16)

    column = lax.broadcasted_iota(jnp.int32, (experts, 2 * experts), 1)
    expert = lax.broadcasted_iota(jnp.int32, (experts, 2 * experts), 0)
    spread = [(column == 2 * expert + h).astype(BF16) for h in range(2)]
    row = lax.broadcasted_iota(jnp.int32, (2 * experts, experts), 0)
    source = lax.broadcasted_iota(jnp.int32, (2 * experts, experts), 1)
    woven = [(row == 2 * source + h).astype(BF16) for h in range(2)]
    mix = [
        [[dot(part, spread[h]).astype(BF16) for part in split(is0 & (c0 == c), is1 & (c1 == c))] for h in range(2)]
        for c in range(CAP)
    ]

    for copy in local:
        copy.wait()
    gates_and_ups.wait_recv()

    own, gathered, here = {}, {}, set()
    low = lax.broadcasted_iota(jnp.int32, (ff, experts), 1) < rows

    def start_partials(k):
        blocks = CHUNKS[k]
        for c in sorted({c for c, _ in blocks} - here):
            await_all(c, a2, yc_peers, A2)
            await_all(c, b2, z_peers, B2)
            here.add(c)
        xa = [
            dot(to_zy[h * rows : (h + 1) * rows], a2[c].reshape(experts, half)).astype(BF16) for c, h in blocks
        ]
        xb = [b2[c, pl.ds(h * side, side)].reshape(rows, half) for c, h in blocks]
        single = len(blocks) == 1
        xa, xb = jnp.concatenate(xa * (1 + single), 0), jnp.concatenate(xb * (1 + single), 0)

        def partial(d):
            both = dot_nt(wg[d, :, :half], xa) + dot_nt(wg[d, :, half:], xb)
            return jnp.where(low, both[:ff], both[ff:]) if single else both

        used = pl.ds(0, ff if single else 2 * ff)
        for device, _, d in x_peers:
            ps[k, d, used] = partial(ntp - d).astype(BF16)
            send(ps.at[k, d, used], pr.at[k, d, used], pair(PS + k), device)
        pending.append(remote(ps.at[k, others, used], pr.at[k, others, used], pair(PS + k), device))
        own[k] = partial(0), pending[-1]

    def finish_partials(k):
        single = len(CHUNKS[k]) == 1
        total, parts = own[k]
        parts.wait_recv()
        for d in range(1, ntp):
            total = total + pr[k, d, pl.ds(0, ff if single else 2 * ff)].astype(F32)
        if single:
            other = jnp.roll(total, rows, 1)
            g, u = jnp.where(low, total, other), jnp.where(low, other, total)
        else:
            g, u = total[:ff], total[ff:]
        h = g / (1.0 + jnp.exp(-g)) * u
        if single:
            h = jnp.where(low[: ff // 2], h[: ff // 2], h[ff // 2 :])
        used = pl.ds(0, h.shape[0])
        hid[k, 0, used] = h.astype(BF16)
        for device, _, d in x_peers:
            send(hid.at[k, 0, used], hid.at[k, d, used], pair(HI + k), device)
        gathered[k] = remote(hid.at[k, others, used], hid.at[k, others, used], pair(HI + k), device)
        pending.append(gathered[k])

    def apply_down(k):
        gathered[k].wait_recv()
        if len(CHUNKS[k]) == 1:
            hidden = dot_nt(same, hid[k, :, pl.ds(0, ff // 2)].reshape(ntp * ff // 2, experts)).astype(BF16)
            first = dn[:, pl.ds(0, ff // 2)].reshape(ntp * ff // 2, share)
            second = dn[:, pl.ds(ff // 2, ff // 2)].reshape(ntp * ff // 2, share)
            result = (dot(hidden[:rows], first) + dot(hidden[rows:], second)).astype(BF16)
        else:
            hidden = dot_nt(same, hid[k].reshape(ntp * ff, experts)).astype(BF16)
            result = dot(hidden, dn[...].reshape(ntp * ff, share)).astype(BF16)
        n = result.shape[0]
        leaving[k, pl.ds(0, n)] = (
            (dot(woven[0][: 2 * n, :n], result[:, :half]) + dot(woven[1][: 2 * n, :n], result[:, half:]))
            .astype(BF16)
            .reshape(n, 2, half)
        )
        for b, (c, h) in enumerate(CHUNKS[k]):
            for j in range(side):
                to_z, first_row = h * side + j, (b * side + j) * nyc

                def give(to_yc, c=c, to_z=to_z, first_row=first_row):
                    send(leaving.at[k, first_row + to_yc], back.at[c, ep], pair(RE + c), (to_z * nyc + to_yc, tp))

                pl.when(z != to_z)(functools.partial(give, yc))

                @pl.when(z == to_z)
                def _(c=c, first_row=first_row):
                    back[c, ep] = leaving[k, first_row + yc]

                for dy, dc in yc_steps:
                    give(yc_to(dy, dc))

    for step, k in ORDER:
        if step == "down" and k == 0:
            downs.wait_recv()
        {"start": start_partials, "finish": finish_partials, "down": apply_down}[step](k)

    sums = [0.0, 0.0]
    for c in range(CAP):
        everything = back.at[c, pl.ds(0, experts - 1)]
        returns = remote(everything, everything, pair(RE + c), x_peers[0][0])
        returns.wait_recv()
        pending.append(returns)
        pairs = back[c].reshape(2 * experts, half)
        for h in range(2):
            for part in mix[c][h]:
                sums[h] = sums[h] + dot(part, pairs)
    out[:, :half] = sums[0].astype(BF16)
    out[:, half:] = sums[1].astype(BF16)

    for copy in pending:
        copy.wait_send()


def body(nz, tokens, norm_gain, routes, group_prob, expert_logits, gate_weight, up_weight, down_matrix):
    tok, width = tokens.shape
    ntp = lax.axis_size("tp")
    nyc = lax.axis_size("ep") // nz
    share, half = width // ntp, width // ntp // 2
    ff = gate_weight.shape[2]
    experts = nz * nyc
    by_z = pltpu.VMEM((CAP, nz, nyc, half), BF16)
    by_yc = pltpu.VMEM((CAP, nyc, nz, half), BF16)
    dma = pltpu.SemaphoreType.DMA
    return pl.pallas_call(
        functools.partial(kernel, nz, nyc, ntp),
        out_shape=jax.ShapeDtypeStruct((tok, share), BF16),
        in_specs=[pl.BlockSpec(memory_space=pltpu.HBM)] * 8,
        out_specs=pl.BlockSpec(memory_space=pltpu.VMEM),
        scratch_shapes=[
            pltpu.VMEM((tok, width), BF16),
            pltpu.VMEM((1, share), F32),
            pltpu.VMEM((2, tok), jnp.int32),
            pltpu.VMEM((1, tok), F32),
            pltpu.VMEM((2, tok), F32),
            pltpu.VMEM((ntp, 2 * ff, share), BF16),
            pltpu.VMEM((ntp, ff, share), BF16),
            by_z, by_yc,
            by_z, by_yc,
            by_yc, by_z,
            by_yc, by_z,
            pltpu.VMEM((NK, ntp, 2 * ff, experts), BF16),
            pltpu.VMEM((NK, ntp, 2 * ff, experts), BF16),
            pltpu.VMEM((NK, ntp, ff, experts), BF16),
            pltpu.VMEM((NK, experts, 2, half), BF16),
            pltpu.VMEM((CAP, experts, 2, half), BF16),
            dma((8,)),
            dma((DN + 1,)), dma((DN + 1,)),
        ],
        compiler_params=pltpu.CompilerParams(
            collective_id=0, has_side_effects=True, vmem_limit_bytes=40 * 2**20
        ),
    )(
        pltpu.with_memory_space_constraint(tokens, pltpu.HBM),
        pltpu.with_memory_space_constraint(norm_gain.reshape(1, width), pltpu.HBM),
        pltpu.with_memory_space_constraint(routes.T, pltpu.HBM),
        pltpu.with_memory_space_constraint(group_prob.reshape(1, tok), pltpu.HBM),
        pltpu.with_memory_space_constraint(expert_logits.T, pltpu.HBM),
        pltpu.with_memory_space_constraint(jnp.swapaxes(gate_weight, 1, 2)[0], pltpu.HBM),
        pltpu.with_memory_space_constraint(jnp.swapaxes(up_weight, 1, 2)[0], pltpu.HBM),
        pltpu.with_memory_space_constraint(down_matrix[0], pltpu.HBM),
    )


def solution(mesh, nz=8):
    return jax.shard_map(
        functools.partial(body, nz),
        mesh=mesh,
        in_specs=(
            P("ep", None),
            P(),
            P("ep", None),
            P("ep"),
            P("ep", None),
            P("ep", None, "tp"),
            P("ep", None, "tp"),
            P("ep", "tp", None),
        ),
        out_specs=P("ep", "tp"),
        check_vma=False,
    )
```

```python
import functools

import jax
import jax.numpy as jnp
from jax import lax
from jax.experimental import pallas as pl
from jax.experimental.pallas import tpu as pltpu
from jax.sharding import PartitionSpec as P

MESH = pl.DeviceIdType.MESH
CAP = 3
CORES = 2
F32, BF16 = jnp.float32, jnp.bfloat16
A1, B1, A2, B2, RE = range(0, 5 * CAP, CAP)
CHUNKS = ((0, 0), (0, 1)), ((1, 0), (2, 0)), ((1, 1),), ((2, 1),)
NK = len(CHUNKS)
ORDER = [
    ("start", 0),
    ("start", 1),
    ("finish", 0),
    ("start", 2),
    ("finish", 1),
    ("start", 3),
    ("down", 0),
    ("down", 1),
    ("finish", 2),
    ("finish", 3),
    ("down", 2),
    ("down", 3),
]
PS, HI, WG = range(5 * CAP, 5 * CAP + 3 * NK, NK)
DN = WG + 1


def quotient(values, divisor):
    return lax.shift_right_logical(values * ((65535 + divisor) // divisor), 16)


def far_first(n):
    return sorted(range(1, n), key=lambda d: -min(d, n - d))


def dot(a, b):
    return jnp.dot(a, b, preferred_element_type=F32)


def dot_nt(a, b):
    return lax.dot_general(a, b, (((1,), (1,)), ((), ())), preferred_element_type=F32)


def kernel(
    nz, nyc, ntp,
    tokens_hbm, gain_hbm, routes_hbm, prob_hbm, logits_hbm, gate, up, down,
    out,
    tokens, gain, routes, prob, logits,
    wg, dn, oa, ob, a1, b1, a1p, b1p, a2, b2, ps, pr, hid, leaving, back,
    lsem, ssem, rsem,
):
    ny = nyc // CORES
    ep, tp = lax.axis_index("ep"), lax.axis_index("tp")
    z, yc = lax.div(ep, nyc), lax.rem(ep, nyc)
    y, core = lax.div(yc, CORES), lax.rem(yc, CORES)
    tok, width = tokens_hbm.shape
    share = width // ntp
    half = share // 2
    ff = gate.shape[0]
    experts = nz * nyc
    side, rows = nz // 2, experts // 2

    z_steps = far_first(nz)
    yc_steps = [(dy, dc) for dy in [*far_first(ny), 0] for dc in range(CORES) if dy or dc]
    x_steps = far_first(ntp)

    def z_to(d):
        return lax.rem(z + d, nz)

    def yc_to(dy, dc):
        return lax.rem(y + dy, ny) * CORES + lax.rem(core + dc, CORES)

    def x_to(d):
        return lax.rem(tp + d, ntp)

    z_peers = [((z_to(d) * nyc + yc, tp), z_to(d), d) for d in z_steps]
    yc_peers = [((z * nyc + yc_to(*d), tp), yc_to(*d), d) for d in yc_steps]
    x_peers = [((ep, x_to(d)), x_to(d), d) for d in x_steps]
    others = pl.ds(1, ntp - 1)

    def columns(j):
        return pl.ds(pl.multiple_of(j * share, share), share)

    inputs = [
        pltpu.make_async_copy(routes_hbm, routes, lsem.at[0]),
        pltpu.make_async_copy(tokens_hbm, tokens, lsem.at[1]),
        pltpu.make_async_copy(gain_hbm.at[:, columns(tp)], gain, lsem.at[2]),
        pltpu.make_async_copy(prob_hbm, prob, lsem.at[3]),
        pltpu.make_async_copy(logits_hbm, logits, lsem.at[4]),
    ]
    for copy in inputs:
        copy.start()

    barrier = pltpu.get_barrier_semaphore()
    for device, *_ in [*z_peers, *yc_peers, *x_peers]:
        pl.semaphore_signal(barrier, inc=1, device_id=device, device_id_type=MESH)

    pending = []

    def remote(src, dst, sems, device):
        return pltpu.make_async_remote_copy(
            src_ref=src, dst_ref=dst, send_sem=sems[0], recv_sem=sems[1], device_id=device, device_id_type=MESH
        )

    def send(src, dst, sems, device):
        remote(src, dst, sems, device).start()

    def pair(number):
        return ssem.at[number], rsem.at[number]

    def exchange(c, src, dst, peers, mine, number):
        sems = pair(number + c)
        for device, there, _ in peers:
            send(src.at[c, there], dst.at[c, mine], sems, device)
        dst[c, mine] = src[c, mine]
        pending.append(remote(src.at[c, pl.ds(0, len(peers))], src.at[c, pl.ds(0, len(peers))], sems, device))

    def await_all(c, dst, peers, number):
        everything = dst.at[c, pl.ds(0, len(peers))]
        remote(everything, everything, pair(number + c), peers[0][0]).wait_recv()

    local = [
        pltpu.make_async_copy(gate.at[:, columns(tp)], wg.at[0, pl.ds(0, ff)], lsem.at[5]),
        pltpu.make_async_copy(up.at[:, columns(tp)], wg.at[0, pl.ds(ff, ff)], lsem.at[6]),
        pltpu.make_async_copy(down.at[:, columns(tp)], dn.at[0], lsem.at[7]),
    ]
    for copy in local:
        copy.start()

    inputs[0].wait()
    r0, r1 = routes[0:1, :], routes[1:2, :]
    ids = lax.broadcasted_iota(jnp.int32, (experts, tok), 0)
    is0, is1 = ids == r0, ids == r1
    e0, e1 = is0.astype(F32), is1.astype(F32)
    before = (
        lax.broadcasted_iota(jnp.int32, (tok, tok), 0) < lax.broadcasted_iota(jnp.int32, (tok, tok), 1)
    ).astype(BF16)
    earlier = dot((e0 + e1).astype(BF16), before)
    c0 = jnp.sum(earlier * e0, 0, keepdims=True)
    c1 = jnp.sum(earlier * e1, 0, keepdims=True)

    def turned(r):
        rz = quotient(r, nyc)
        return (r - rz * nyc) * nz + rz

    is0b, is1b = ids == turned(r0), ids == turned(r1)

    inputs[1].wait()
    inputs[2].wait()
    values = tokens[...].astype(F32)
    scale = lax.rsqrt(jnp.sum(values * values, -1, keepdims=True) * (1.0 / width) + 1e-06)
    normed = (tokens[:, columns(tp)].astype(F32) * scale * gain[...]).astype(BF16)

    for c in range(CAP):
        in0, in1 = c0 == c, c1 == c
        pick = ((is0 & in0) | (is1 & in1)).astype(BF16)
        oa[c] = dot(pick, normed[:, :half]).astype(BF16).reshape(oa.shape[1:])
        pick = ((is0b & in0) | (is1b & in1)).astype(BF16)
        ob[c] = dot(pick, normed[:, half:]).astype(BF16).reshape(ob.shape[1:])

    pl.semaphore_wait(barrier, len(z_peers) + len(yc_peers) + len(x_peers))

    for c in range(CAP):
        exchange(c, oa, a1, z_peers, z, A1)
        exchange(c, ob, b1, yc_peers, yc, B1)
        if c == 0:
            for device, there, d in x_peers:
                send(gate.at[:, columns(there)], wg.at[d, pl.ds(0, ff)], pair(WG), device)
                send(up.at[:, columns(there)], wg.at[d, pl.ds(ff, ff)], pair(WG), device)
            gates_and_ups = remote(wg.at[others], wg.at[others], pair(WG), device)
    for device, there, d in x_peers:
        send(down.at[:, columns(there)], dn.at[d], pair(DN), device)
    downs = remote(dn.at[others], dn.at[others], pair(DN), device)
    pending += [gates_and_ups, downs]

    to = lax.broadcasted_iota(jnp.int32, (experts, experts), 0)
    of = lax.broadcasted_iota(jnp.int32, (experts, experts), 1)

    def reorder(outer, inner):
        i = quotient(to, inner)
        return (of == (to - i * inner) * outer + i).astype(BF16)

    to_yz, to_zy = reorder(nyc, nz), reorder(nz, nyc)
    same = (of == to).astype(BF16)

    def reordered(c, matrix, src, dst):
        dst[c] = dot(matrix, src[c].reshape(experts, half)).astype(BF16).reshape(dst.shape[1:])

    for c in range(CAP):
        await_all(c, a1, z_peers, A1)
        reordered(c, to_yz, a1, a1p)
        exchange(c, a1p, a2, yc_peers, yc, A2)
        await_all(c, b1, yc_peers, B1)
        reordered(c, to_zy, b1, b1p)
        exchange(c, b1p, b2, z_peers, z, B2)

    inputs[3].wait()
    inputs[4].wait()
    top = jnp.maximum(logits[0:1, :], logits[1:2, :])
    x0, x1 = jnp.exp(logits[0:1, :] - top), jnp.exp(logits[1:2, :] - top)
    w0, w1 = prob[...] * (x0 / (x0 + x1)), prob[...] * (x1 / (x0 + x1))
    zero = jnp.zeros((experts, tok), F32)

    def split(at0, at1):
        whole = (jnp.where(at0, w0, zero) + jnp.where(at1, w1, zero)).T
        high = whole.astype(BF16)
        return high, (whole - high.astype(F32)).astype(BF16)

    column = lax.broadcasted_iota(jnp.int32, (experts, 2 * experts), 1)
    expert = lax.broadcasted_iota(jnp.int32, (experts, 2 * experts), 0)
    spread = [(column == 2 * expert + h).astype(BF16) for h in range(2)]
    row = lax.broadcasted_iota(jnp.int32, (2 * experts, experts), 0)
    source = lax.broadcasted_iota(jnp.int32, (2 * experts, experts), 1)
    woven = [(row == 2 * source + h).astype(BF16) for h in range(2)]
    mix = [
        [[dot(part, spread[h]).astype(BF16) for part in split(is0 & (c0 == c), is1 & (c1 == c))] for h in range(2)]
        for c in range(CAP)
    ]

    for copy in local:
        copy.wait()
    gates_and_ups.wait_recv()

    own, gathered, here = {}, {}, set()
    low = lax.broadcasted_iota(jnp.int32, (ff, experts), 1) < rows

    def start_partials(k):
        blocks = CHUNKS[k]
        for c in sorted({c for c, _ in blocks} - here):
            await_all(c, a2, yc_peers, A2)
            await_all(c, b2, z_peers, B2)
            here.add(c)
        xa = [
            dot(to_zy[h * rows : (h + 1) * rows], a2[c].reshape(experts, half)).astype(BF16) for c, h in blocks
        ]
        xb = [b2[c, pl.ds(h * side, side)].reshape(rows, half) for c, h in blocks]
        single = len(blocks) == 1
        xa, xb = jnp.concatenate(xa * (1 + single), 0), jnp.concatenate(xb * (1 + single), 0)

        def partial(d):
            both = dot_nt(wg[d, :, :half], xa) + dot_nt(wg[d, :, half:], xb)
            return jnp.where(low, both[:ff], both[ff:]) if single else both

        used = pl.ds(0, ff if single else 2 * ff)
        for device, _, d in x_peers:
            ps[k, d, used] = partial(ntp - d).astype(BF16)
            send(ps.at[k, d, used], pr.at[k, d, used], pair(PS + k), device)
        pending.append(remote(ps.at[k, others, used], pr.at[k, others, used], pair(PS + k), device))
        own[k] = partial(0), pending[-1]

    def finish_partials(k):
        single = len(CHUNKS[k]) == 1
        total, parts = own[k]
        parts.wait_recv()
        for d in range(1, ntp):
            total = total + pr[k, d, pl.ds(0, ff if single else 2 * ff)].astype(F32)
        if single:
            other = jnp.roll(total, rows, 1)
            g, u = jnp.where(low, total, other), jnp.where(low, other, total)
        else:
            g, u = total[:ff], total[ff:]
        h = g / (1.0 + jnp.exp(-g)) * u
        if single:
            h = jnp.where(low[: ff // 2], h[: ff // 2], h[ff // 2 :])
        used = pl.ds(0, h.shape[0])
        hid[k, 0, used] = h.astype(BF16)
        for device, _, d in x_peers:
            send(hid.at[k, 0, used], hid.at[k, d, used], pair(HI + k), device)
        gathered[k] = remote(hid.at[k, others, used], hid.at[k, others, used], pair(HI + k), device)
        pending.append(gathered[k])

    def apply_down(k):
        gathered[k].wait_recv()
        if len(CHUNKS[k]) == 1:
            hidden = dot_nt(same, hid[k, :, pl.ds(0, ff // 2)].reshape(ntp * ff // 2, experts)).astype(BF16)
            first = dn[:, pl.ds(0, ff // 2)].reshape(ntp * ff // 2, share)
            second = dn[:, pl.ds(ff // 2, ff // 2)].reshape(ntp * ff // 2, share)
            result = (dot(hidden[:rows], first) + dot(hidden[rows:], second)).astype(BF16)
        else:
            hidden = dot_nt(same, hid[k].reshape(ntp * ff, experts)).astype(BF16)
            result = dot(hidden, dn[...].reshape(ntp * ff, share)).astype(BF16)
        n = result.shape[0]
        leaving[k, pl.ds(0, n)] = (
            (dot(woven[0][: 2 * n, :n], result[:, :half]) + dot(woven[1][: 2 * n, :n], result[:, half:]))
            .astype(BF16)
            .reshape(n, 2, half)
        )
        for b, (c, h) in enumerate(CHUNKS[k]):
            for j in range(side):
                to_z, first_row = h * side + j, (b * side + j) * nyc

                def give(to_yc, c=c, to_z=to_z, first_row=first_row):
                    send(leaving.at[k, first_row + to_yc], back.at[c, ep], pair(RE + c), (to_z * nyc + to_yc, tp))

                pl.when(z != to_z)(functools.partial(give, yc))

                @pl.when(z == to_z)
                def _(c=c, first_row=first_row):
                    back[c, ep] = leaving[k, first_row + yc]

                for dy, dc in yc_steps:
                    give(yc_to(dy, dc))

    for step, k in ORDER:
        if step == "down" and k == 0:
            downs.wait_recv()
        {"start": start_partials, "finish": finish_partials, "down": apply_down}[step](k)

    sums = [0.0, 0.0]
    for c in range(CAP):
        everything = back.at[c, pl.ds(0, experts - 1)]
        returns = remote(everything, everything, pair(RE + c), x_peers[0][0])
        returns.wait_recv()
        pending.append(returns)
        pairs = back[c].reshape(2 * experts, half)
        for h in range(2):
            for part in mix[c][h]:
                sums[h] = sums[h] + dot(part, pairs)
    out[:, :half] = sums[0].astype(BF16)
    out[:, half:] = sums[1].astype(BF16)

    for copy in pending:
        copy.wait_send()


def body(nz, tokens, norm_gain, routes, group_prob, expert_logits, gate_weight, up_weight, down_matrix):
    tok, width = tokens.shape
    ntp = lax.axis_size("tp")
    nyc = lax.axis_size("ep") // nz
    share, half = width // ntp, width // ntp // 2
    ff = gate_weight.shape[2]
    experts = nz * nyc
    by_z = pltpu.VMEM((CAP, nz, nyc, half), BF16)
    by_yc = pltpu.VMEM((CAP, nyc, nz, half), BF16)
    dma = pltpu.SemaphoreType.DMA
    return pl.pallas_call(
        functools.partial(kernel, nz, nyc, ntp),
        out_shape=jax.ShapeDtypeStruct((tok, share), BF16),
        in_specs=[pl.BlockSpec(memory_space=pltpu.HBM)] * 8,
        out_specs=pl.BlockSpec(memory_space=pltpu.VMEM),
        scratch_shapes=[
            pltpu.VMEM((tok, width), BF16),
            pltpu.VMEM((1, share), F32),
            pltpu.VMEM((2, tok), jnp.int32),
            pltpu.VMEM((1, tok), F32),
            pltpu.VMEM((2, tok), F32),
            pltpu.VMEM((ntp, 2 * ff, share), BF16),
            pltpu.VMEM((ntp, ff, share), BF16),
            by_z, by_yc,
            by_z, by_yc,
            by_yc, by_z,
            by_yc, by_z,
            pltpu.VMEM((NK, ntp, 2 * ff, experts), BF16),
            pltpu.VMEM((NK, ntp, 2 * ff, experts), BF16),
            pltpu.VMEM((NK, ntp, ff, experts), BF16),
            pltpu.VMEM((NK, experts, 2, half), BF16),
            pltpu.VMEM((CAP, experts, 2, half), BF16),
            dma((8,)),
            dma((DN + 1,)), dma((DN + 1,)),
        ],
        compiler_params=pltpu.CompilerParams(
            collective_id=0, has_side_effects=True, vmem_limit_bytes=40 * 2**20
        ),
    )(
        pltpu.with_memory_space_constraint(tokens, pltpu.HBM),
        pltpu.with_memory_space_constraint(norm_gain.reshape(1, width), pltpu.HBM),
        pltpu.with_memory_space_constraint(routes.T, pltpu.HBM),
        pltpu.with_memory_space_constraint(group_prob.reshape(1, tok), pltpu.HBM),
        pltpu.with_memory_space_constraint(expert_logits.T, pltpu.HBM),
        pltpu.with_memory_space_constraint(jnp.swapaxes(gate_weight, 1, 2)[0], pltpu.HBM),
        pltpu.with_memory_space_constraint(jnp.swapaxes(up_weight, 1, 2)[0], pltpu.HBM),
        pltpu.with_memory_space_constraint(down_matrix[0], pltpu.HBM),
    )


def solution(mesh, nz=8):
    return jax.shard_map(
        functools.partial(body, nz),
        mesh=mesh,
        in_specs=(
            P("ep", None),
            P(),
            P("ep", None),
            P("ep"),
            P("ep", None),
            P("ep", None, "tp"),
            P("ep", None, "tp"),
            P("ep", "tp", None),
        ),
        out_specs=P("ep", "tp"),
        check_vma=False,
    )
```

```python
import functools

import jax
import jax.numpy as jnp
from jax import lax
from jax.experimental import pallas as pl
from jax.experimental.pallas import tpu as pltpu
from jax.sharding import PartitionSpec as P

MESH = pl.DeviceIdType.MESH
CAP = 3
CORES = 2
F32, BF16 = jnp.float32, jnp.bfloat16
A1, B1, A2, B2, RE = range(0, 5 * CAP, CAP)
CHUNKS = ((0, 0), (0, 1)), ((1, 0), (2, 0)), ((1, 1),), ((2, 1),)
NK = len(CHUNKS)
ORDER = [
    ("start", 0),
    ("start", 1),
    ("finish", 0),
    ("start", 2),
    ("finish", 1),
    ("start", 3),
    ("down", 0),
    ("down", 1),
    ("finish", 2),
    ("finish", 3),
    ("down", 2),
    ("down", 3),
]
PS, HI, WG = range(5 * CAP, 5 * CAP + 3 * NK, NK)
DN = WG + 1


def quotient(values, divisor):
    return lax.shift_right_logical(values * ((65535 + divisor) // divisor), 16)


def far_first(n):
    return sorted(range(1, n), key=lambda d: -min(d, n - d))


def dot(a, b):
    return jnp.dot(a, b, preferred_element_type=F32)


def dot_nt(a, b):
    return lax.dot_general(a, b, (((1,), (1,)), ((), ())), preferred_element_type=F32)


def kernel(
    nz, nyc, ntp,
    tokens_hbm, gain_hbm, routes_hbm, prob_hbm, logits_hbm, gate, up, down,
    out,
    tokens, gain, routes, prob, logits,
    wg, dn, oa, ob, a1, b1, a1p, b1p, a2, b2, ps, pr, hid, leaving, back,
    lsem, ssem, rsem,
):
    ny = nyc // CORES
    ep, tp = lax.axis_index("ep"), lax.axis_index("tp")
    z, yc = lax.div(ep, nyc), lax.rem(ep, nyc)
    y, core = lax.div(yc, CORES), lax.rem(yc, CORES)
    tok, width = tokens_hbm.shape
    share = width // ntp
    half = share // 2
    ff = gate.shape[0]
    experts = nz * nyc
    side, rows = nz // 2, experts // 2

    z_steps = far_first(nz)
    yc_steps = [(dy, dc) for dy in [*far_first(ny), 0] for dc in range(CORES) if dy or dc]
    x_steps = far_first(ntp)

    def z_to(d):
        return lax.rem(z + d, nz)

    def yc_to(dy, dc):
        return lax.rem(y + dy, ny) * CORES + lax.rem(core + dc, CORES)

    def x_to(d):
        return lax.rem(tp + d, ntp)

    z_peers = [((z_to(d) * nyc + yc, tp), z_to(d), d) for d in z_steps]
    yc_peers = [((z * nyc + yc_to(*d), tp), yc_to(*d), d) for d in yc_steps]
    x_peers = [((ep, x_to(d)), x_to(d), d) for d in x_steps]
    others = pl.ds(1, ntp - 1)

    def columns(j):
        return pl.ds(pl.multiple_of(j * share, share), share)

    inputs = [
        pltpu.make_async_copy(routes_hbm, routes, lsem.at[0]),
        pltpu.make_async_copy(tokens_hbm, tokens, lsem.at[1]),
        pltpu.make_async_copy(gain_hbm.at[:, columns(tp)], gain, lsem.at[2]),
        pltpu.make_async_copy(prob_hbm, prob, lsem.at[3]),
        pltpu.make_async_copy(logits_hbm, logits, lsem.at[4]),
    ]
    for copy in inputs:
        copy.start()

    barrier = pltpu.get_barrier_semaphore()
    for device, *_ in [*z_peers, *yc_peers, *x_peers]:
        pl.semaphore_signal(barrier, inc=1, device_id=device, device_id_type=MESH)

    pending = []

    def remote(src, dst, sems, device):
        return pltpu.make_async_remote_copy(
            src_ref=src, dst_ref=dst, send_sem=sems[0], recv_sem=sems[1], device_id=device, device_id_type=MESH
        )

    def send(src, dst, sems, device):
        remote(src, dst, sems, device).start()

    def pair(number):
        return ssem.at[number], rsem.at[number]

    def exchange(c, src, dst, peers, mine, number):
        sems = pair(number + c)
        for device, there, _ in peers:
            send(src.at[c, there], dst.at[c, mine], sems, device)
        dst[c, mine] = src[c, mine]
        pending.append(remote(src.at[c, pl.ds(0, len(peers))], src.at[c, pl.ds(0, len(peers))], sems, device))

    def await_all(c, dst, peers, number):
        everything = dst.at[c, pl.ds(0, len(peers))]
        remote(everything, everything, pair(number + c), peers[0][0]).wait_recv()

    local = [
        pltpu.make_async_copy(gate.at[:, columns(tp)], wg.at[0, pl.ds(0, ff)], lsem.at[5]),
        pltpu.make_async_copy(up.at[:, columns(tp)], wg.at[0, pl.ds(ff, ff)], lsem.at[6]),
        pltpu.make_async_copy(down.at[:, columns(tp)], dn.at[0], lsem.at[7]),
    ]
    for copy in local:
        copy.start()

    inputs[0].wait()
    r0, r1 = routes[0:1, :], routes[1:2, :]
    ids = lax.broadcasted_iota(jnp.int32, (experts, tok), 0)
    is0, is1 = ids == r0, ids == r1
    e0, e1 = is0.astype(F32), is1.astype(F32)
    before = (
        lax.broadcasted_iota(jnp.int32, (tok, tok), 0) < lax.broadcasted_iota(jnp.int32, (tok, tok), 1)
    ).astype(BF16)
    earlier = dot((e0 + e1).astype(BF16), before)
    c0 = jnp.sum(earlier * e0, 0, keepdims=True)
    c1 = jnp.sum(earlier * e1, 0, keepdims=True)

    def turned(r):
        rz = quotient(r, nyc)
        return (r - rz * nyc) * nz + rz

    is0b, is1b = ids == turned(r0), ids == turned(r1)

    inputs[1].wait()
    inputs[2].wait()
    values = tokens[...].astype(F32)
    scale = lax.rsqrt(jnp.sum(values * values, -1, keepdims=True) * (1.0 / width) + 1e-06)
    normed = (tokens[:, columns(tp)].astype(F32) * scale * gain[...]).astype(BF16)

    for c in range(CAP):
        in0, in1 = c0 == c, c1 == c
        pick = ((is0 & in0) | (is1 & in1)).astype(BF16)
        oa[c] = dot(pick, normed[:, :half]).astype(BF16).reshape(oa.shape[1:])
        pick = ((is0b & in0) | (is1b & in1)).astype(BF16)
        ob[c] = dot(pick, normed[:, half:]).astype(BF16).reshape(ob.shape[1:])

    pl.semaphore_wait(barrier, len(z_peers) + len(yc_peers) + len(x_peers))

    for device, there, d in x_peers:
        send(gate.at[:, columns(there)], wg.at[d, pl.ds(0, ff)], pair(WG), device)
        send(up.at[:, columns(there)], wg.at[d, pl.ds(ff, ff)], pair(WG), device)
    gates_and_ups = remote(wg.at[others], wg.at[others], pair(WG), device)
    for c in range(CAP):
        exchange(c, oa, a1, z_peers, z, A1)
        exchange(c, ob, b1, yc_peers, yc, B1)
    for device, there, d in x_peers:
        send(down.at[:, columns(there)], dn.at[d], pair(DN), device)
    downs = remote(dn.at[others], dn.at[others], pair(DN), device)
    pending += [gates_and_ups, downs]

    to = lax.broadcasted_iota(jnp.int32, (experts, experts), 0)
    of = lax.broadcasted_iota(jnp.int32, (experts, experts), 1)

    def reorder(outer, inner):
        i = quotient(to, inner)
        return (of == (to - i * inner) * outer + i).astype(BF16)

    to_yz, to_zy = reorder(nyc, nz), reorder(nz, nyc)
    same = (of == to).astype(BF16)

    def reordered(c, matrix, src, dst):
        dst[c] = dot(matrix, src[c].reshape(experts, half)).astype(BF16).reshape(dst.shape[1:])

    for c in range(CAP):
        await_all(c, a1, z_peers, A1)
        reordered(c, to_yz, a1, a1p)
        exchange(c, a1p, a2, yc_peers, yc, A2)
        await_all(c, b1, yc_peers, B1)
        reordered(c, to_zy, b1, b1p)
        exchange(c, b1p, b2, z_peers, z, B2)

    inputs[3].wait()
    inputs[4].wait()
    top = jnp.maximum(logits[0:1, :], logits[1:2, :])
    x0, x1 = jnp.exp(logits[0:1, :] - top), jnp.exp(logits[1:2, :] - top)
    w0, w1 = prob[...] * (x0 / (x0 + x1)), prob[...] * (x1 / (x0 + x1))
    zero = jnp.zeros((experts, tok), F32)

    def split(at0, at1):
        whole = (jnp.where(at0, w0, zero) + jnp.where(at1, w1, zero)).T
        high = whole.astype(BF16)
        return high, (whole - high.astype(F32)).astype(BF16)

    column = lax.broadcasted_iota(jnp.int32, (experts, 2 * experts), 1)
    expert = lax.broadcasted_iota(jnp.int32, (experts, 2 * experts), 0)
    spread = [(column == 2 * expert + h).astype(BF16) for h in range(2)]
    row = lax.broadcasted_iota(jnp.int32, (2 * experts, experts), 0)
    source = lax.broadcasted_iota(jnp.int32, (2 * experts, experts), 1)
    woven = [(row == 2 * source + h).astype(BF16) for h in range(2)]
    mix = [
        [[dot(part, spread[h]).astype(BF16) for part in split(is0 & (c0 == c), is1 & (c1 == c))] for h in range(2)]
        for c in range(CAP)
    ]

    for copy in local:
        copy.wait()
    gates_and_ups.wait_recv()

    own, gathered, here = {}, {}, set()
    low = lax.broadcasted_iota(jnp.int32, (ff, experts), 1) < rows

    def start_partials(k):
        blocks = CHUNKS[k]
        for c in sorted({c for c, _ in blocks} - here):
            await_all(c, a2, yc_peers, A2)
            await_all(c, b2, z_peers, B2)
            here.add(c)
        xa = [
            dot(to_zy[h * rows : (h + 1) * rows], a2[c].reshape(experts, half)).astype(BF16) for c, h in blocks
        ]
        xb = [b2[c, pl.ds(h * side, side)].reshape(rows, half) for c, h in blocks]
        single = len(blocks) == 1
        xa, xb = jnp.concatenate(xa * (1 + single), 0), jnp.concatenate(xb * (1 + single), 0)

        def partial(d):
            both = dot_nt(wg[d, :, :half], xa) + dot_nt(wg[d, :, half:], xb)
            return jnp.where(low, both[:ff], both[ff:]) if single else both

        used = pl.ds(0, ff if single else 2 * ff)
        for device, _, d in x_peers:
            ps[k, d, used] = partial(ntp - d).astype(BF16)
            send(ps.at[k, d, used], pr.at[k, d, used], pair(PS + k), device)
        pending.append(remote(ps.at[k, others, used], pr.at[k, others, used], pair(PS + k), device))
        own[k] = partial(0), pending[-1]

    def finish_partials(k):
        single = len(CHUNKS[k]) == 1
        total, parts = own[k]
        parts.wait_recv()
        for d in range(1, ntp):
            total = total + pr[k, d, pl.ds(0, ff if single else 2 * ff)].astype(F32)
        if single:
            other = jnp.roll(total, rows, 1)
            g, u = jnp.where(low, total, other), jnp.where(low, other, total)
        else:
            g, u = total[:ff], total[ff:]
        h = g / (1.0 + jnp.exp(-g)) * u
        if single:
            h = jnp.where(low[: ff // 2], h[: ff // 2], h[ff // 2 :])
        used = pl.ds(0, h.shape[0])
        hid[k, 0, used] = h.astype(BF16)
        for device, _, d in x_peers:
            send(hid.at[k, 0, used], hid.at[k, d, used], pair(HI + k), device)
        gathered[k] = remote(hid.at[k, others, used], hid.at[k, others, used], pair(HI + k), device)
        pending.append(gathered[k])

    def apply_down(k):
        gathered[k].wait_recv()
        if len(CHUNKS[k]) == 1:
            hidden = dot_nt(same, hid[k, :, pl.ds(0, ff // 2)].reshape(ntp * ff // 2, experts)).astype(BF16)
            first = dn[:, pl.ds(0, ff // 2)].reshape(ntp * ff // 2, share)
            second = dn[:, pl.ds(ff // 2, ff // 2)].reshape(ntp * ff // 2, share)
            result = (dot(hidden[:rows], first) + dot(hidden[rows:], second)).astype(BF16)
        else:
            hidden = dot_nt(same, hid[k].reshape(ntp * ff, experts)).astype(BF16)
            result = dot(hidden, dn[...].reshape(ntp * ff, share)).astype(BF16)
        n = result.shape[0]
        leaving[k, pl.ds(0, n)] = (
            (dot(woven[0][: 2 * n, :n], result[:, :half]) + dot(woven[1][: 2 * n, :n], result[:, half:]))
            .astype(BF16)
            .reshape(n, 2, half)
        )
        targets = [(h * side + j, b * side + j, c) for b, (c, h) in enumerate(CHUNKS[k]) for j in range(side)]
        for to_z, group, c in sorted(targets):
            first_row = group * nyc

            def give(to_yc, c=c, to_z=to_z, first_row=first_row):
                send(leaving.at[k, first_row + to_yc], back.at[c, ep], pair(RE + c), (to_z * nyc + to_yc, tp))

            pl.when(z != to_z)(functools.partial(give, yc))

            @pl.when(z == to_z)
            def _(c=c, first_row=first_row):
                back[c, ep] = leaving[k, first_row + yc]

            for dy, dc in yc_steps:
                give(yc_to(dy, dc))

    for step, k in ORDER:
        if step == "down" and k == 0:
            downs.wait_recv()
        {"start": start_partials, "finish": finish_partials, "down": apply_down}[step](k)

    sums = [0.0, 0.0]
    for c in range(CAP):
        everything = back.at[c, pl.ds(0, experts - 1)]
        returns = remote(everything, everything, pair(RE + c), x_peers[0][0])
        returns.wait_recv()
        pending.append(returns)
        pairs = back[c].reshape(2 * experts, half)
        for h in range(2):
            for part in mix[c][h]:
                sums[h] = sums[h] + dot(part, pairs)
    out[:, :half] = sums[0].astype(BF16)
    out[:, half:] = sums[1].astype(BF16)

    for copy in pending:
        copy.wait_send()


def body(nz, tokens, norm_gain, routes, group_prob, expert_logits, gate_weight, up_weight, down_matrix):
    tok, width = tokens.shape
    ntp = lax.axis_size("tp")
    nyc = lax.axis_size("ep") // nz
    share, half = width // ntp, width // ntp // 2
    ff = gate_weight.shape[2]
    experts = nz * nyc
    by_z = pltpu.VMEM((CAP, nz, nyc, half), BF16)
    by_yc = pltpu.VMEM((CAP, nyc, nz, half), BF16)
    dma = pltpu.SemaphoreType.DMA
    return pl.pallas_call(
        functools.partial(kernel, nz, nyc, ntp),
        out_shape=jax.ShapeDtypeStruct((tok, share), BF16),
        in_specs=[pl.BlockSpec(memory_space=pltpu.HBM)] * 8,
        out_specs=pl.BlockSpec(memory_space=pltpu.VMEM),
        scratch_shapes=[
            pltpu.VMEM((tok, width), BF16),
            pltpu.VMEM((1, share), F32),
            pltpu.VMEM((2, tok), jnp.int32),
            pltpu.VMEM((1, tok), F32),
            pltpu.VMEM((2, tok), F32),
            pltpu.VMEM((ntp, 2 * ff, share), BF16),
            pltpu.VMEM((ntp, ff, share), BF16),
            by_z, by_yc,
            by_z, by_yc,
            by_yc, by_z,
            by_yc, by_z,
            pltpu.VMEM((NK, ntp, 2 * ff, experts), BF16),
            pltpu.VMEM((NK, ntp, 2 * ff, experts), BF16),
            pltpu.VMEM((NK, ntp, ff, experts), BF16),
            pltpu.VMEM((NK, experts, 2, half), BF16),
            pltpu.VMEM((CAP, experts, 2, half), BF16),
            dma((8,)),
            dma((DN + 1,)), dma((DN + 1,)),
        ],
        compiler_params=pltpu.CompilerParams(
            collective_id=0, has_side_effects=True, vmem_limit_bytes=40 * 2**20
        ),
    )(
        pltpu.with_memory_space_constraint(tokens, pltpu.HBM),
        pltpu.with_memory_space_constraint(norm_gain.reshape(1, width), pltpu.HBM),
        pltpu.with_memory_space_constraint(routes.T, pltpu.HBM),
        pltpu.with_memory_space_constraint(group_prob.reshape(1, tok), pltpu.HBM),
        pltpu.with_memory_space_constraint(expert_logits.T, pltpu.HBM),
        pltpu.with_memory_space_constraint(jnp.swapaxes(gate_weight, 1, 2)[0], pltpu.HBM),
        pltpu.with_memory_space_constraint(jnp.swapaxes(up_weight, 1, 2)[0], pltpu.HBM),
        pltpu.with_memory_space_constraint(down_matrix[0], pltpu.HBM),
    )


def solution(mesh, nz=8):
    return jax.shard_map(
        functools.partial(body, nz),
        mesh=mesh,
        in_specs=(
            P("ep", None),
            P(),
            P("ep", None),
            P("ep"),
            P("ep", None),
            P("ep", None, "tp"),
            P("ep", None, "tp"),
            P("ep", "tp", None),
        ),
        out_specs=P("ep", "tp"),
        check_vma=False,
    )
```
